512 devices in a mesh: dp: 4 (over x), kv: 64 (over z, y), tp: 2 (over core).
Axes of the slice: x: 4, y: 8, z: 8, core: 2. Of those that a mesh axis runs over, the one named last changes fastest.
Arguments:
- tokens: bfloat16 [64, 16, 2048], P('dp'), may hold values from -6 to 6
- norm_gain: float32 [2048], replicated, may hold values from 0.1 to 1.9
- query_weight: bfloat16 [2048, 1024], P(None, 'tp'), may hold values from -0.125 to 0.125
- key_weight: bfloat16 [2048, 256], P(None, 'tp'), may hold values from -0.125 to 0.125
- value_weight: bfloat16 [2048, 256], P(None, 'tp'), may hold values from -0.125 to 0.125
- forget_weight: bfloat16 [2048, 8], replicated, may hold values from -0.125 to 0.125
- forget_bias: float32 [8], replicated, may hold values from 0 to 4
- query_gain: float32 [128], replicated, may hold values from 0.1 to 1.9
- key_gain: float32 [128], replicated, may hold values from 0.1 to 1.9
- output_weight: bfloat16 [1024, 2048], P('tp', 'kv'), may hold values from -0.1875 to 0.1875
- cache_keys: bfloat16 [64, 16384, 2, 128], P('dp', 'kv', 'tp'), may hold values from -512 to 512
- cache_values: bfloat16 [64, 16384, 2, 128], P('dp', 'kv', 'tp'), may hold values from -6 to 6
- cache_logcum: float32 [64, 16384, 8], P('dp', 'kv', 'tp'), may hold values from -3277 to 0, as said below
- pending_keys: bfloat16 [64, 4, 2, 128], P('dp', None, 'tp'), may hold values from -6 to 6
- pending_values: bfloat16 [64, 4, 2, 128], P('dp', None, 'tp'), may hold values from -6 to 6
- pending_logcum: float32 [64, 4, 8], P('dp', None, 'tp'), may hold values from -3277 to 0, as said below
- lengths: int32 [64], P('dp'), may hold values from 8192 to 16380, as said below
- accepted: int32 [64], P('dp'), may hold values from 1 to 4
- parents: int32 [64, 16], P('dp'), may hold values from -1 to 14, as said below
Outputs:
- result: bfloat16 [64, 16, 2048], P('dp', None, ('kv', 'tp'))
The draws below stay inside these ranges and needn't reach their ends.
Inputs may be any that keep to these rules, and one draw needn't show every extreme that they name: Positions below lengths hold a sequence's past; the last step's accepted proposals go to positions lengths to lengths + accepted - 1. `parents`: the parent of proposal i is -1 (the last accepted token) or a proposal before i. `cache_logcum`: non-increasing along positions for every sequence and head. `pending_logcum`: the cumulative log gates at positions lengths to lengths + 3, continuing cache_logcum.
All inputs are finite; a program needn't handle non-finite values.
Results may differ from the reference program's by a relative error of at most 0.014.
Values may be sent and summed in bfloat16 or wider, within the bound.
A program may use at most 128 MiB of HBM per device.

```python
import math
import jax
import jax.numpy as jnp
from jax import lax

D = 2048
HEADS = 8
KV_HEADS = 2
HEAD_DIM = 128
PROP = 16
ACC_MAX = 4
POS_DEV = 256
SEQUENCE_COUNT = 64
LEN = 16384
BLOCKS = 64
GROUPS = 2
Q_WIDTH = 1024
KV_WIDTH = 256


def gate_tables(key):
    overall_length = LEN + ACC_MAX
    lengths = jax.random.randint(jax.random.fold_in(key, 101), (SEQUENCE_COUNT,), LEN // 2, LEN - ACC_MAX + 1, dtype=jnp.int32)
    head_order = jax.random.permutation(jax.random.fold_in(key, 102), HEADS)
    fast_count = HEADS // 2
    quick_fading_heads = (head_order < fast_count).astype(jnp.float32)
    slow_rate = jnp.exp(jax.random.uniform(jax.random.fold_in(key, 103), (SEQUENCE_COUNT, 1, HEADS), jnp.float32, math.log(0.2), math.log(0.8))) / LEN
    fast_rate = jnp.exp(jax.random.uniform(jax.random.fold_in(key, 104), (SEQUENCE_COUNT, 1, HEADS), jnp.float32, math.log(0.01), math.log(1.0 / 30.0)))
    fading_speed = quick_fading_heads * fast_rate + (1.0 - quick_fading_heads) * slow_rate
    block_count = overall_length // POS_DEV + 1
    block_spread = jnp.exp(jax.random.uniform(jax.random.fold_in(key, 105), (SEQUENCE_COUNT, block_count, HEADS), jnp.float32, math.log(0.4), math.log(2.5)))
    token_place = jnp.arange(overall_length, dtype=jnp.int32)
    block_lookup = block_spread[:, token_place // POS_DEV, :]
    jaggedness = jnp.exp(jax.random.uniform(jax.random.fold_in(key, 106), (SEQUENCE_COUNT, overall_length, HEADS), jnp.float32, math.log(0.5), math.log(2.0)))
    spike_location = jax.random.randint(jax.random.fold_in(key, 107), (SEQUENCE_COUNT, 3), 0, overall_length, dtype=jnp.int32)
    spike_magnitude = jax.random.uniform(jax.random.fold_in(key, 108), (SEQUENCE_COUNT, 3), jnp.float32, 0.22, 0.6)
    spike_penalty = jnp.sum((token_place[None, None, :] == spike_location[:, :, None]).astype(jnp.float32) * spike_magnitude[:, :, None], axis=1)
    length_steps = fading_speed * block_lookup * jaggedness + spike_penalty[:, :, None] * (1.0 - quick_fading_heads)
    return (lengths, -jnp.cumsum(length_steps, axis=1))


def draw_lengths(key, part):
    lengths, cumulative = gate_tables(key)
    return lengths


def draw_cache_logcum(key, part):
    lengths, cumulative = gate_tables(key)
    return cumulative[:, :LEN, :].astype(jnp.float32)


def draw_pending_logcum(key, part):
    lengths, cumulative = gate_tables(key)
    indices = lengths[:, None] + jnp.arange(ACC_MAX, dtype=jnp.int32)[None, :]
    return jnp.take_along_axis(cumulative, indices[:, :, None], axis=1).astype(jnp.float32)


def draw_parents(key, part):
    bounds = jnp.arange(PROP, dtype=jnp.int32)[None, :]
    return jax.random.randint(key, (SEQUENCE_COUNT, PROP), -1, bounds, dtype=jnp.int32)


def draw_cache_keys(key, part):
    shape = (SEQUENCE_COUNT, LEN, KV_HEADS, HEAD_DIM)
    drawn = jnp.clip(jax.random.normal(jax.random.fold_in(key, 201), shape, jnp.float32), -6.0, 6.0)
    return drawn.astype(jnp.bfloat16)


def with_ends(values, stream_key, least, largest):
    index_at = [jax.random.randint(jax.random.fold_in(stream_key, axis), (), 0, length) for axis, length in enumerate(values.shape)]
    main_axis = values.shape.index(max(values.shape))
    next_to = index_at[:main_axis] + [(index_at[main_axis] + 1) % values.shape[main_axis]] + index_at[main_axis + 1:]
    return values.at[tuple(index_at)].set(least).at[tuple(next_to)].set(largest)


def level_of(key, extent, pieces, smallest, largest):
    gain = 1.0
    for dim, shards_of in pieces:
        heights = jax.random.uniform(jax.random.fold_in(jax.random.fold_in(key, 6), dim), (shards_of,), jnp.float32, smallest / len(pieces), largest / len(pieces))
        gain = gain * jnp.repeat(jnp.exp(heights), extent[dim] // shards_of).reshape((-1,) + (1,) * (len(extent) - 1 - dim))
    return gain


def centred(own_key, extent, width, reach, shards=(), kind=jnp.bfloat16):
    array = jax.random.normal(own_key, extent, jnp.float32) * width
    if len(shards) > 0:
        array = level_of(own_key, extent, shards, -0.22, 0.18) * array
    return jnp.clip(array, min=-reach, max=reach).astype(kind)


def setup_inputs(seed: int = 0) -> dict:
    streams_of = jax.random.split(jax.random.key(seed), 20)
    return {
        "tokens": centred(streams_of[0], (SEQUENCE_COUNT, PROP, D), 1.0, 6.0, ((0, 4),)),
        "norm_gain": jnp.clip(1.0 + 0.18 * jax.random.normal(streams_of[1], (D,), jnp.float32), 0.1, 1.9),
        "query_weight": centred(streams_of[2], (D, Q_WIDTH), D ** -0.5, 0.125, ((1, 2),)),
        "key_weight": centred(streams_of[3], (D, KV_WIDTH), D ** -0.5, 0.125, ((1, 2),)),
        "value_weight": centred(streams_of[4], (D, KV_WIDTH), D ** -0.5, 0.125, ((1, 2),)),
        "forget_weight": centred(streams_of[5], (D, HEADS), D ** -0.5, 0.125),
        "forget_bias": jnp.clip(jax.random.uniform(streams_of[6], (HEADS,), jnp.float32, 0.0, 4.0), 0.0, 4.0),
        "query_gain": jnp.clip(1.0 + 0.18 * jax.random.normal(streams_of[7], (HEAD_DIM,), jnp.float32), 0.1, 1.9),
        "key_gain": jnp.clip(1.0 + 0.18 * jax.random.normal(streams_of[8], (HEAD_DIM,), jnp.float32), 0.1, 1.9),
        "output_weight": centred(streams_of[9], (Q_WIDTH, D), Q_WIDTH ** -0.5, 0.1875, ((0, 2), (1, 64))),
        "cache_keys": draw_cache_keys(jax.random.fold_in(streams_of[19], 71), 0),
        "cache_values": centred(streams_of[11], (SEQUENCE_COUNT, LEN, KV_HEADS, HEAD_DIM), 1.0, 6.0, ((0, 4), (1, 64), (2, 2))),
        "cache_logcum": draw_cache_logcum(jax.random.fold_in(streams_of[19], 71), 0),
        "pending_keys": centred(streams_of[13], (SEQUENCE_COUNT, ACC_MAX, KV_HEADS, HEAD_DIM), 1.0, 6.0, ((0, 4), (2, 2))),
        "pending_values": centred(streams_of[14], (SEQUENCE_COUNT, ACC_MAX, KV_HEADS, HEAD_DIM), 1.0, 6.0, ((0, 4), (2, 2))),
        "pending_logcum": draw_pending_logcum(jax.random.fold_in(streams_of[19], 71), 0),
        "lengths": draw_lengths(jax.random.fold_in(streams_of[19], 71), 0),
        "accepted": with_ends(jax.random.randint(streams_of[17], (SEQUENCE_COUNT,), 1, ACC_MAX + 1), jax.random.fold_in(streams_of[17], 1), 1, ACC_MAX).astype(jnp.int32),
        "parents": draw_parents(jax.random.fold_in(streams_of[19], 71), 0),
    }


EPSILON = 1e-06
NEG_LARGE = -1e+30
HIGHEST = lax.Precision.HIGHEST

def head_norm(vectors, gain_vec):
    return vectors * lax.rsqrt(lax.optimization_barrier(jnp.mean(vectors * vectors, axis=-1, keepdims=True)) + EPSILON) * gain_vec

def ancestors(parents):
    node_count = parents.shape[-1]
    indices = jnp.arange(node_count, dtype=jnp.int32)
    reachable = (parents[..., None] == indices).astype(jnp.float32) + jnp.eye(node_count, dtype=jnp.float32)
    for doubling in range((node_count - 1).bit_length()):
        reachable = jnp.minimum(jnp.einsum('sij,sjk->sik', reachable, reachable, precision=HIGHEST), 1.0)
    return reachable

def one_sequence(inputs):
    query_rows, key_rows, value_rows, cumulative, ancestry, cache_k, cache_v, cache_l, pend_k, pend_v, pend_l, length_now, taken_now = inputs
    sharing = HEADS // KV_HEADS
    scaling = HEAD_DIM ** (-0.5)
    token_place = jnp.arange(LEN, dtype=jnp.int32)
    offset = token_place - length_now
    inserted = (offset >= 0) & (offset < taken_now)
    one_hot = ((offset[:, None] == jnp.arange(ACC_MAX, dtype=jnp.int32)[None, :]) & inserted[:, None]).astype(jnp.float32)
    all_keys = jnp.where(inserted[:, None, None], jnp.einsum('la,akd->lkd', one_hot, pend_k.astype(jnp.float32), precision=HIGHEST), cache_k.astype(jnp.float32))
    all_values = jnp.where(inserted[:, None, None], jnp.einsum('la,akd->lkd', one_hot, pend_v.astype(jnp.float32), precision=HIGHEST), cache_v.astype(jnp.float32))
    all_logcum = jnp.where(inserted[:, None], jnp.einsum('la,ah->lh', one_hot, pend_l, precision=HIGHEST), cache_l)
    usable = token_place < length_now + taken_now
    query_group = query_rows.astype(jnp.float32).reshape(PROP, KV_HEADS, sharing, HEAD_DIM)
    scores = jnp.einsum('pkgd,lkd->kgpl', query_group, all_keys, precision=HIGHEST).reshape(HEADS, PROP, LEN)
    scores = scores * scaling + cumulative.T[:, :, None] - all_logcum.T[:, None, :]
    blocked = scores.reshape(HEADS, PROP, BLOCKS, POS_DEV)
    visible = usable.reshape(BLOCKS, POS_DEV)[None, None]
    block_max = lax.optimization_barrier(jnp.max(jnp.where(visible, blocked, NEG_LARGE), axis=-1))
    weights = jnp.where(visible, jnp.exp(blocked - block_max[..., None]), 0.0)
    block_sum = lax.optimization_barrier(jnp.sum(weights, axis=-1))
    rounded = lax.optimization_barrier(weights.astype(jnp.bfloat16)).astype(jnp.float32)
    rounded = rounded.reshape(KV_HEADS, sharing, PROP, BLOCKS, POS_DEV)
    block_values = jnp.einsum('kgpnl,nlkd->kgpnd', rounded, all_values.reshape(BLOCKS, POS_DEV, KV_HEADS, HEAD_DIM), precision=HIGHEST)
    block_values = block_values.reshape(HEADS, PROP, BLOCKS, HEAD_DIM)
    tree_scores = jnp.einsum('pkgd,jkd->kgpj', query_group, key_rows.astype(jnp.float32), precision=HIGHEST).reshape(HEADS, PROP, PROP)
    tree_scores = tree_scores * scaling + cumulative.T[:, :, None] - cumulative.T[:, None, :]
    tree_mask = ancestry[None] > 0.5
    tree_max = lax.optimization_barrier(jnp.max(jnp.where(tree_mask, tree_scores, NEG_LARGE), axis=-1))
    tree_weights = jnp.where(tree_mask, jnp.exp(tree_scores - tree_max[..., None]), 0.0)
    tree_sum = lax.optimization_barrier(jnp.sum(tree_weights, axis=-1))
    tree_rounded = lax.optimization_barrier(tree_weights.astype(jnp.bfloat16)).astype(jnp.float32)
    tree_values = jnp.einsum('kgpj,jkd->kgpd', tree_rounded.reshape(KV_HEADS, sharing, PROP, PROP), value_rows.astype(jnp.float32), precision=HIGHEST).reshape(HEADS, PROP, HEAD_DIM)
    overall = jnp.maximum(lax.optimization_barrier(jnp.max(block_max, axis=-1)), tree_max)
    factor_cache = jnp.exp(block_max - overall[..., None])
    factor_tree = jnp.exp(tree_max - overall)
    denominator = lax.optimization_barrier(jnp.sum(block_sum * factor_cache, axis=-1)) + tree_sum * factor_tree
    numerator = lax.optimization_barrier(jnp.sum(block_values * factor_cache[..., None], axis=2)) + tree_values * factor_tree[..., None]
    return jnp.transpose(numerator / denominator[..., None], (1, 0, 2)).astype(jnp.bfloat16)

def reference(tokens, norm_gain, query_weight, key_weight, value_weight, forget_weight, forget_bias, query_gain, key_gain, output_weight, cache_keys, cache_values, cache_logcum, pending_keys, pending_values, pending_logcum, lengths, accepted, parents):
    seq_count, node_count, model_width = tokens.shape
    widened = tokens.astype(jnp.float32)
    normed = (widened * lax.rsqrt(lax.optimization_barrier(jnp.mean(widened * widened, axis=-1, keepdims=True)) + EPSILON) * norm_gain).astype(jnp.bfloat16)
    token_rows = normed.reshape(seq_count * node_count, model_width)
    query_raw = jnp.dot(token_rows, query_weight, preferred_element_type=jnp.float32)
    key_raw = jnp.dot(token_rows, key_weight, preferred_element_type=jnp.float32)
    value_raw = jnp.dot(token_rows, value_weight, preferred_element_type=jnp.float32)
    queries = head_norm(query_raw.reshape(seq_count, node_count, HEADS, HEAD_DIM), query_gain).astype(jnp.bfloat16)
    keys_new = head_norm(key_raw.reshape(seq_count, node_count, KV_HEADS, HEAD_DIM), key_gain).astype(jnp.bfloat16)
    values_new = value_raw.reshape(seq_count, node_count, KV_HEADS, HEAD_DIM).astype(jnp.bfloat16)
    log_gates = jax.nn.log_sigmoid(jnp.dot(token_rows, forget_weight, preferred_element_type=jnp.float32) + forget_bias).reshape(seq_count, node_count, HEADS)
    ancestry = ancestors(parents)
    choose = (jnp.arange(ACC_MAX, dtype=jnp.int32)[None, :] == (accepted - 1)[:, None]).astype(jnp.float32)
    base_gate = jnp.einsum('sa,sah->sh', choose, pending_logcum, precision=HIGHEST)
    cumulative = base_gate[:, None, :] + jnp.einsum('sij,sjh->sih', ancestry, log_gates, precision=HIGHEST)
    attended = lax.map(one_sequence, (queries, keys_new, values_new, cumulative, ancestry, cache_keys, cache_values, cache_logcum, pending_keys, pending_values, pending_logcum, lengths, accepted))
    grouped = attended.reshape(seq_count, node_count, GROUPS, Q_WIDTH // GROUPS).astype(jnp.float32)
    out_rows = output_weight.reshape(GROUPS, Q_WIDTH // GROUPS, model_width).astype(jnp.float32)
    head_part = jnp.einsum('spgc,gcd->gspd', grouped, out_rows, precision=HIGHEST).astype(jnp.bfloat16)
    return lax.optimization_barrier(jnp.sum(head_part.astype(jnp.float32), axis=0)).astype(jnp.bfloat16)
```

```python
import functools

import jax
import jax.numpy as jnp
from jax import lax
from jax.experimental import pallas as pl
from jax.experimental.pallas import tpu as pltpu
from jax.sharding import PartitionSpec as P

EPSILON = 1e-06
NEG_LARGE = -1e30
NEG_FLOOR = -1e29
HIGHEST = lax.Precision.HIGHEST
MESH = pl.DeviceIdType.MESH
F32 = jnp.float32
BF16 = jnp.bfloat16
LAST = (((1,), (1,)), ((), ()))


def iota(shape, dim):
    return lax.broadcasted_iota(jnp.int32, shape, dim)


def dot_last(a, b):
    return lax.dot_general(a, b, LAST, preferred_element_type=F32)


def unit(rows, gain):
    return rows * lax.rsqrt(jnp.mean(rows * rows, axis=-1, keepdims=True) + EPSILON) * gain


def kernel(
    seqs,
    heads,
    props,
    head,
    taken,
    block,
    tokens_hbm,
    norm_gain,
    query_hbm,
    key_hbm,
    value_hbm,
    forget,
    forget_bias,
    query_gain,
    key_gain,
    out_weight,
    keys_hbm,
    values_hbm,
    logcum,
    pending_keys,
    pending_values,
    pending_logcum,
    lengths,
    accepted,
    accepted_row,
    parents,
    result,
    tok,
    normed,
    wq,
    wk,
    wv,
    kbuf,
    vbuf,
    q_scr,
    kn_scr,
    vn_scr,
    anc_scr,
    cum_scr,
    o_send,
    o_recv,
    lse_send,
    lse_recv,
    tree_scr,
    att,
    swap_send,
    swap_recv,
    load_sem,
    send_sem,
    recv_sem,
):
    rows = seqs * props
    peers = seqs * heads
    scaling = head**-0.5
    me = lax.axis_index("kv")
    core = lax.axis_index("tp")
    my_seq = me // heads
    my_head = me % heads

    def load(src, dst, n):
        return pltpu.make_async_copy(src, dst, load_sem.at[n])

    loads = [
        load(tokens_hbm, tok, 0),
        load(key_hbm, wk, 1),
        load(value_hbm, wv, 2),
        load(query_hbm, wq, 3),
        load(keys_hbm, kbuf, 4),
        load(values_hbm, vbuf, 5),
    ]
    for item in loads:
        item.start()

    barrier = pltpu.get_barrier_semaphore()

    @pl.loop(1, peers)
    def _(step):
        pl.semaphore_signal(
            barrier, inc=1, device_id={"kv": (me + step) % peers}, device_id_type=MESH
        )

    pl.semaphore_signal(barrier, inc=1, device_id={"tp": 1 - core}, device_id_type=MESH)

    lane = iota((seqs, rows), 1)
    spread = ((iota((props, rows), 1) & (props - 1)) == iota((props, rows), 0)).astype(BF16)
    repeated = jnp.dot(
        parents[...].astype(F32).astype(BF16), spread, preferred_element_type=F32
    )
    parent_row = jnp.sum(
        jnp.where(lane // props == iota((seqs, rows), 0), repeated, 0.0), axis=0, keepdims=True
    ).astype(jnp.int32)
    down = iota((rows, rows), 0)
    across = iota((rows, rows), 1)
    same = down // props == across // props
    linked = (same & (parent_row == (down & (props - 1)))) | (down == across)
    anc_t = jnp.where(linked, 1.0, 0.0).astype(BF16)
    for _ in range((props - 1).bit_length()):
        anc_t = jnp.minimum(jnp.dot(anc_t, anc_t, preferred_element_type=F32), 1.0).astype(BF16)
    anc_scr[...] = anc_t

    loads[0].wait()

    @pl.loop(0, rows // 16)
    def _(step):
        piece = pl.ds(step * 16, 16)
        wide = tok[piece, :].astype(F32)
        normed[piece, :] = unit(wide, norm_gain[...]).astype(BF16)

    gate_raw = dot_last(forget[...], normed[...])
    gate_head = iota((2 * heads, 1), 0)
    bias = jnp.zeros((2 * heads, 1), F32)
    for n in range(2 * heads):
        bias = jnp.where(gate_head == n, forget_bias[n], bias)
    gate_raw = gate_raw + bias
    gates = jnp.minimum(gate_raw, 0.0) - jnp.log1p(jnp.exp(-jnp.abs(gate_raw)))
    gates = jnp.where(
        core == 0, gates, jnp.concatenate([gates[heads:], gates[:heads]], axis=0)
    )
    base = jnp.zeros((heads, seqs), F32)
    for a in range(taken):
        base = jnp.where(accepted_row[...] - 1 == a, pending_logcum[a], base)
    base = jnp.concatenate([base, jnp.zeros((heads, seqs), F32)], axis=0)
    expand = (lane // props == iota((seqs, rows), 0)).astype(F32)
    cum_t = jnp.dot(
        gates, anc_t.astype(F32), precision=HIGHEST, preferred_element_type=F32
    ) + jnp.dot(base, expand, precision=HIGHEST, preferred_element_type=F32)
    cum_scr[...] = cum_t.T

    loads[1].wait()
    kn_scr[...] = unit(
        jnp.dot(normed[...], wk[...], preferred_element_type=F32), key_gain[...]
    ).astype(BF16)
    loads[2].wait()
    vn_scr[...] = jnp.dot(normed[...], wv[...], preferred_element_type=F32).astype(BF16)
    loads[3].wait()
    for h in range(heads):
        raw = jnp.dot(
            normed[...], wq[:, h * head : (h + 1) * head], preferred_element_type=F32
        )
        q_scr[:, h * props : (h + 1) * props, :] = (
            unit(raw, query_gain[...]).astype(BF16).reshape(seqs, props, head)
        )

    o_recv[pl.ds(peers, 8)] = jnp.zeros((8, props, head), BF16)
    lse_recv[pl.ds(peers, 8)] = jnp.full((8, 1, 128), NEG_LARGE, F32)

    loads[4].wait()
    loads[5].wait()
    pl.semaphore_wait(barrier, peers)

    def send_out(k):
        return pltpu.make_async_remote_copy(
            src_ref=o_send.at[k],
            dst_ref=o_recv.at[me],
            send_sem=send_sem.at[0],
            recv_sem=recv_sem.at[0],
            device_id={"kv": k},
            device_id_type=MESH,
        )

    def send_lse(k):
        return pltpu.make_async_remote_copy(
            src_ref=lse_send.at[k // heads],
            dst_ref=lse_recv.at[me],
            send_sem=send_sem.at[1],
            recv_sem=recv_sem.at[1],
            device_id={"kv": k},
            device_id_type=MESH,
        )

    def send_att(k):
        mine = att.at[my_head * seqs + my_seq]
        return pltpu.make_async_remote_copy(
            src_ref=mine,
            dst_ref=mine,
            send_sem=send_sem.at[2],
            recv_sem=recv_sem.at[2],
            device_id={"kv": k},
            device_id_type=MESH,
        )

    def all_but_one(ref, n):
        some = ref.at[pl.ds(0, peers - 1)]
        return pltpu.make_async_remote_copy(
            src_ref=some,
            dst_ref=some,
            send_sem=send_sem.at[n],
            recv_sem=recv_sem.at[n],
            device_id={"kv": me},
            device_id_type=MESH,
        )

    planes = seqs // 2
    my_plane = my_seq // 2
    place = me * block + iota((1, block), 1)

    @pl.loop(0, planes // 2, init_carry=jnp.zeros((heads * props, 128), F32))
    def lse_cols(g, cols):
        members = []
        for far in (planes // 2 + g, planes // 2 - 1 - g):
            plane = (my_plane + far) % planes
            members += [2 * plane, 2 * plane + 1]
        for s in members:
            raw = dot_last(q_scr[s], kbuf[s])
            minus = jnp.where(place < lengths[s], -logcum[s], NEG_LARGE)
            cum = cum_scr[pl.ds(pl.multiple_of(s * props, props), props), :]
            scores = jnp.concatenate(
                [
                    raw[h * props : (h + 1) * props] * scaling
                    + (cum[:, h : h + 1] + minus[h : h + 1])
                    for h in range(heads)
                ],
                axis=0,
            )
            top = jnp.maximum(jnp.max(scores, axis=-1, keepdims=True), NEG_FLOOR)
            weights = jnp.exp(scores - top)
            total = jnp.sum(weights, axis=-1, keepdims=True)
            some = total > 0.0
            safe = jnp.where(some, total, 1.0)
            out = jnp.dot(weights.astype(BF16), vbuf[s], preferred_element_type=F32)
            out = (out * (1.0 / safe)).astype(BF16)
            o_send[pl.ds(s * heads, heads)] = out.reshape(heads, props, head)
            lse = jnp.where(some, top + jnp.log(safe), NEG_LARGE)
            cols = jnp.where(iota((heads * props, 128), 1) == s, lse, cols)
        for s in members:
            for h in range(heads):
                k = s * heads + h

                @pl.when(k != me)
                def _():
                    send_out(k).start()

                @pl.when(k == me)
                def _():
                    o_recv[me] = o_send[k]

        return cols

    padded = jnp.concatenate([lse_cols, jnp.zeros((128 - heads * props, 128), F32)], axis=0)
    lse_rows = padded.T
    for s in range(seqs):
        lse_send[s] = lse_rows[s : s + 1]
    lse_recv[me] = lse_send[my_seq]

    @pl.loop(1, peers)
    def _(step):
        send_lse((me + step) % peers).start()

    width = heads * props
    q_own = q_scr[my_seq]
    own_rows = pl.ds(pl.multiple_of(my_seq * props, props), props)
    extra = 16
    pad = jnp.zeros((extra - taken, head), F32)
    keys_x = jnp.concatenate(
        [
            kn_scr[own_rows, :].astype(F32),
            pending_keys[my_seq].astype(F32),
            pad,
        ],
        axis=0,
    ).astype(BF16)
    values_x = jnp.concatenate(
        [
            vn_scr[own_rows, :].astype(F32),
            pending_values[my_seq].astype(F32),
            pad,
        ],
        axis=0,
    ).astype(BF16)
    raw_t = dot_last(keys_x, q_own)
    cum_own = cum_scr[own_rows, :]
    lane_head = iota((props, width), 1) // props
    lane_prop = iota((props, width), 1) & (props - 1)
    cum_wide = jnp.zeros((props, width), F32)
    for h in range(heads):
        cum_wide = jnp.where(lane_head == h, cum_own[:, h : h + 1], cum_wide)
    cum_row = jnp.sum(
        jnp.where(lane_prop == iota((props, width), 0), cum_wide, 0.0), axis=0, keepdims=True
    )
    anc_fold = (
        (iota((rows, width), 0) & (props - 1)) == (iota((rows, width), 1) & (props - 1))
    ).astype(BF16)
    anc_own = jnp.dot(anc_scr[own_rows, :], anc_fold, preferred_element_type=F32)
    pend_wide = jnp.zeros((extra, width), F32)
    pend_sub = iota((extra, width), 0)
    for a in range(taken):
        col = jnp.sum(
            jnp.where(iota((heads, seqs), 1) == my_seq, pending_logcum[a], 0.0),
            axis=1,
            keepdims=True,
        )
        row = jnp.sum(
            jnp.where(iota((heads, width), 1) // props == iota((heads, width), 0), col, 0.0),
            axis=0,
            keepdims=True,
        )
        pend_wide = jnp.where(pend_sub == a, row, pend_wide)
    tree_t = jnp.where(
        anc_own > 0.5, raw_t[:props] * scaling + cum_row - cum_wide, NEG_LARGE
    )
    pend_t = jnp.where(
        pend_sub < accepted[my_seq], raw_t[props:] * scaling + cum_row - pend_wide, NEG_LARGE
    )
    both_t = jnp.concatenate([tree_t, pend_t], axis=0)
    top_t = jnp.max(both_t, axis=0, keepdims=True)
    weights_t = jnp.exp(both_t - top_t)
    total_t = jnp.sum(weights_t, axis=0, keepdims=True)
    share_t = (weights_t * (1.0 / total_t)).astype(BF16)
    tree_scr[...] = lax.dot_general(
        share_t, values_x, (((0,), (0,)), ((), ())), preferred_element_type=F32
    )
    head_rows = pl.ds(pl.multiple_of(my_head * props, props), props)
    o_recv[peers] = tree_scr[head_rows, :].astype(BF16)
    lse_t = top_t + jnp.log(total_t)
    lse_recv[peers] = jnp.concatenate([lse_t, jnp.zeros((1, 128 - width), F32)], axis=1)

    all_but_one(lse_recv, 1).wait_recv()
    slots = peers + 8
    lse_all = lse_recv[:, 0, :]
    weight = jnp.exp(lse_all - jnp.max(lse_all, axis=0, keepdims=True)).astype(BF16)
    pick = (
        (iota((128, 128), 0) - my_head * props) == (iota((128, 128), 1) & (props - 1))
    ).astype(BF16)
    picked = jnp.dot(weight, pick, preferred_element_type=F32)
    mine_8 = iota((8, 128), 1) // props == iota((8, 128), 0)
    mine_16 = (iota((props, 128), 1) & (props - 1)) == iota((props, 128), 0)
    mixes = []
    for c in range(slots // 8):
        flat = jnp.sum(
            jnp.where(mine_8, picked[c * 8 : (c + 1) * 8], 0.0), axis=0, keepdims=True
        )
        mixes.append(jnp.where(mine_16, flat, 0.0))
    den = functools.reduce(lambda a, b: a + b, mixes)
    den = jnp.sum(den, axis=1, keepdims=True)
    mix = jnp.concatenate(mixes, axis=1).astype(BF16)
    all_but_one(o_recv, 0).wait_recv()
    blended = jnp.dot(
        mix, o_recv[...].reshape(slots * props, head), preferred_element_type=F32
    )
    att[my_head * seqs + my_seq] = (blended / den).astype(BF16)

    @pl.loop(1, peers)
    def _(step):
        send_att((me + step) % peers).start()

    all_but_one(att, 2).wait_recv()

    part_t = jnp.zeros((out_weight.shape[0], rows), F32)
    for h in range(heads):
        part_t += dot_last(
            out_weight[:, h * head : (h + 1) * head],
            att[pl.ds(h * seqs, seqs)].reshape(rows, head),
        )
    half = out_weight.shape[0] // 2
    low, high = part_t[:half].astype(BF16), part_t[half:].astype(BF16)
    swap_send[...] = jnp.where(core == 0, high, low)
    swap = pltpu.make_async_remote_copy(
        src_ref=swap_send,
        dst_ref=swap_recv,
        send_sem=send_sem.at[3],
        recv_sem=recv_sem.at[3],
        device_id={"tp": 1 - core},
        device_id_type=MESH,
    )
    swap.start()
    kept = jnp.where(core == 0, low, high).astype(F32)
    swap.wait()
    final = kept + swap_recv[...].astype(F32)
    result[...] = final.T.astype(BF16).reshape(seqs, props, half)

    all_but_one(o_send, 0).wait_send()
    all_but_one(lse_recv, 1).wait_send()
    all_but_one(att, 2).wait_send()


def shards(
    tokens,
    norm_gain,
    query_weight,
    key_weight,
    value_weight,
    forget_weight,
    forget_bias,
    query_gain,
    key_gain,
    output_weight,
    cache_keys,
    cache_values,
    cache_logcum,
    pending_keys,
    pending_values,
    pending_logcum,
    lengths,
    accepted,
    parents,
):
    seqs, props, width = tokens.shape
    head = query_gain.shape[0]
    heads = query_weight.shape[1] // head
    block = cache_keys.shape[1]
    taken = pending_keys.shape[1]
    rows = seqs * props
    peers = seqs * heads
    half = output_weight.shape[1] // 2
    whole = pl.BlockSpec(memory_space=pltpu.VMEM)
    scalars = pl.BlockSpec(memory_space=pltpu.SMEM)
    stay = pl.BlockSpec(memory_space=pl.ANY)
    operands = [
        (tokens.reshape(rows, width), stay),
        (norm_gain.reshape(1, width), whole),
        (query_weight, stay),
        (key_weight, stay),
        (value_weight, stay),
        (forget_weight.T, whole),
        (forget_bias, scalars),
        (query_gain.reshape(1, head), whole),
        (key_gain.reshape(1, head), whole),
        (output_weight.T, whole),
        (cache_keys.reshape(seqs, block, head), stay),
        (cache_values.reshape(seqs, block, head), stay),
        (jnp.swapaxes(cache_logcum, 1, 2), whole),
        (pending_keys.reshape(seqs, taken, head), whole),
        (pending_values.reshape(seqs, taken, head), whole),
        (jnp.transpose(pending_logcum, (1, 2, 0)), whole),
        (lengths, scalars),
        (accepted, scalars),
        (accepted.reshape(1, seqs), whole),
        (parents, whole),
    ]
    return pl.pallas_call(
        functools.partial(kernel, seqs, heads, props, head, taken, block),
        out_shape=jax.ShapeDtypeStruct((seqs, props, half), BF16),
        in_specs=[spec for _, spec in operands],
        out_specs=whole,
        scratch_shapes=[
            pltpu.VMEM((rows, width), BF16),
            pltpu.VMEM((rows, width), BF16),
            pltpu.VMEM((width, heads * head), BF16),
            pltpu.VMEM((width, head), BF16),
            pltpu.VMEM((width, head), BF16),
            pltpu.VMEM((seqs, block, head), BF16),
            pltpu.VMEM((seqs, block, head), BF16),
            pltpu.VMEM((seqs, heads * props, head), BF16),
            pltpu.VMEM((rows, head), BF16),
            pltpu.VMEM((rows, head), BF16),
            pltpu.VMEM((rows, rows), BF16),
            pltpu.VMEM((rows, 2 * heads), F32),
            pltpu.VMEM((peers, props, head), BF16),
            pltpu.VMEM((peers + 8, props, head), BF16),
            pltpu.VMEM((seqs, 1, 128), F32),
            pltpu.VMEM((peers + 8, 1, 128), F32),
            pltpu.VMEM((heads * props, head), F32),
            pltpu.VMEM((peers, props, head), BF16),
            pltpu.VMEM((half, rows), BF16),
            pltpu.VMEM((half, rows), BF16),
            pltpu.SemaphoreType.DMA((6,)),
            pltpu.SemaphoreType.DMA((4,)),
            pltpu.SemaphoreType.DMA((4,)),
        ],
        compiler_params=pltpu.CompilerParams(
            collective_id=0, has_side_effects=True, vmem_limit_bytes=48 * 1024 * 1024
        ),
    )(*[array for array, _ in operands])


def solution(mesh):
    placed = (
        P("dp", None, None),
        P(),
        P(None, "tp"),
        P(None, "tp"),
        P(None, "tp"),
        P(),
        P(),
        P(),
        P(),
        P("tp", "kv"),
        P("dp", "kv", "tp", None),
        P("dp", "kv", "tp", None),
        P("dp", "kv", "tp"),
        P("dp", None, "tp", None),
        P("dp", None, "tp", None),
        P("dp", None, "tp"),
        P("dp"),
        P("dp"),
        P("dp", None),
    )
    return jax.shard_map(
        shards, mesh=mesh, in_specs=placed, out_specs=P("dp", None, ("kv", "tp")), check_vma=False
    )
```

```python
import functools

import jax
import jax.numpy as jnp
from jax import lax
from jax.experimental import pallas as pl
from jax.experimental.pallas import tpu as pltpu
from jax.sharding import PartitionSpec as P

EPSILON = 1e-06
NEG_LARGE = -1e30
NEG_FLOOR = -1e29
HIGHEST = lax.Precision.HIGHEST
MESH = pl.DeviceIdType.MESH
F32 = jnp.float32
BF16 = jnp.bfloat16
LAST = (((1,), (1,)), ((), ()))
NAMES = (
    "tokens",
    "norm_gain",
    "query_weight",
    "key_weight",
    "value_weight",
    "forget",
    "forget_bias",
    "query_gain",
    "key_gain",
    "out_weight",
    "keys",
    "values",
    "logcum",
    "pending_keys",
    "pending_values",
    "pending_logcum",
    "lengths",
    "accepted",
    "accepted_row",
    "parents",
)
SCALARS = ("forget_bias", "lengths", "accepted")
LOAD_ORDER = (
    "parents",
    "tokens",
    "norm_gain",
    "forget",
    "forget_bias",
    "accepted_row",
    "pending_logcum",
    "key_gain",
    "query_gain",
    "key_weight",
    "value_weight",
    "query_weight",
    "keys",
    "logcum",
    "lengths",
    "values",
    "accepted",
    "pending_keys",
    "pending_values",
    "out_weight",
)


def iota(shape, dim):
    return lax.broadcasted_iota(jnp.int32, shape, dim)


def dot_last(a, b):
    return lax.dot_general(a, b, LAST, preferred_element_type=F32)


def unit(rows, gain):
    return rows * lax.rsqrt(jnp.mean(rows * rows, axis=-1, keepdims=True) + EPSILON) * gain


def kernel(
    seqs,
    heads,
    props,
    head,
    taken,
    block,
    operands,
    result,
    places,
    normed,
    q_scr,
    kn_scr,
    vn_scr,
    anc_scr,
    cum_scr,
    o_send,
    o_recv,
    lse_send,
    lse_recv,
    tree_scr,
    att,
    swap_send,
    swap_recv,
    load_sem,
    send_sem,
    recv_sem,
):
    rows = seqs * props
    peers = seqs * heads
    scaling = head**-0.5
    me = lax.axis_index("kv")
    core = lax.axis_index("tp")
    my_seq = me // heads
    my_head = me % heads

    loads = {
        name: pltpu.make_async_copy(operands[name], places[name], load_sem.at[n])
        for n, name in enumerate(LOAD_ORDER)
    }
    for item in loads.values():
        item.start()
    (
        tok, norm_gain, wq, wk, wv, forget, forget_bias, query_gain, key_gain, out_weight,
        kbuf, vbuf, logcum, pending_keys, pending_values, pending_logcum, lengths, accepted,
        accepted_row, parents,
    ) = (places[name] for name in NAMES)

    barrier = pltpu.get_barrier_semaphore()

    @pl.loop(1, peers)
    def _(step):
        pl.semaphore_signal(
            barrier, inc=1, device_id={"kv": (me + step) % peers}, device_id_type=MESH
        )

    pl.semaphore_signal(barrier, inc=1, device_id={"tp": 1 - core}, device_id_type=MESH)

    loads["parents"].wait()

    lane = iota((seqs, rows), 1)
    spread = ((iota((props, rows), 1) & (props - 1)) == iota((props, rows), 0)).astype(BF16)
    repeated = jnp.dot(
        parents[...].astype(F32).astype(BF16), spread, preferred_element_type=F32
    )
    parent_row = jnp.sum(
        jnp.where(lane // props == iota((seqs, rows), 0), repeated, 0.0), axis=0, keepdims=True
    ).astype(jnp.int32)
    down = iota((rows, rows), 0)
    across = iota((rows, rows), 1)
    same = down // props == across // props
    linked = (same & (parent_row == (down & (props - 1)))) | (down == across)
    anc_t = jnp.where(linked, 1.0, 0.0).astype(BF16)
    for _ in range((props - 1).bit_length()):
        anc_t = jnp.minimum(jnp.dot(anc_t, anc_t, preferred_element_type=F32), 1.0).astype(BF16)
    anc_scr[...] = anc_t

    loads["tokens"].wait()
    loads["norm_gain"].wait()

    @pl.loop(0, rows // 16)
    def _(step):
        piece = pl.ds(step * 16, 16)
        wide = tok[piece, :].astype(F32)
        normed[piece, :] = unit(wide, norm_gain[...]).astype(BF16)

    for name in ("forget", "forget_bias", "accepted_row", "pending_logcum"):
        loads[name].wait()
    gate_raw = dot_last(forget[...], normed[...])
    gate_head = iota((2 * heads, 1), 0)
    bias = jnp.zeros((2 * heads, 1), F32)
    for n in range(2 * heads):
        bias = jnp.where(gate_head == n, forget_bias[n], bias)
    gate_raw = gate_raw + bias
    gates = jnp.minimum(gate_raw, 0.0) - jnp.log1p(jnp.exp(-jnp.abs(gate_raw)))
    gates = jnp.where(
        core == 0, gates, jnp.concatenate([gates[heads:], gates[:heads]], axis=0)
    )
    base = jnp.zeros((heads, seqs), F32)
    for a in range(taken):
        base = jnp.where(accepted_row[...] - 1 == a, pending_logcum[a], base)
    base = jnp.concatenate([base, jnp.zeros((heads, seqs), F32)], axis=0)
    expand = (lane // props == iota((seqs, rows), 0)).astype(F32)
    cum_t = jnp.dot(
        gates, anc_t.astype(F32), precision=HIGHEST, preferred_element_type=F32
    ) + jnp.dot(base, expand, precision=HIGHEST, preferred_element_type=F32)
    cum_scr[...] = cum_t.T

    loads["key_gain"].wait()
    loads["key_weight"].wait()
    kn_scr[...] = unit(
        jnp.dot(normed[...], wk[...], preferred_element_type=F32), key_gain[...]
    ).astype(BF16)
    loads["value_weight"].wait()
    vn_scr[...] = jnp.dot(normed[...], wv[...], preferred_element_type=F32).astype(BF16)
    loads["query_gain"].wait()
    loads["query_weight"].wait()
    for h in range(heads):
        raw = jnp.dot(
            normed[...], wq[:, h * head : (h + 1) * head], preferred_element_type=F32
        )
        q_scr[:, h * props : (h + 1) * props, :] = (
            unit(raw, query_gain[...]).astype(BF16).reshape(seqs, props, head)
        )

    o_recv[pl.ds(peers, 8)] = jnp.zeros((8, props, head), BF16)
    lse_recv[pl.ds(peers, 8)] = jnp.full((8, 1, 128), NEG_LARGE, F32)

    for name in ("keys", "logcum", "lengths", "values"):
        loads[name].wait()
    pl.semaphore_wait(barrier, peers)

    def send_out(k):
        return pltpu.make_async_remote_copy(
            src_ref=o_send.at[k],
            dst_ref=o_recv.at[me],
            send_sem=send_sem.at[0],
            recv_sem=recv_sem.at[0],
            device_id={"kv": k},
            device_id_type=MESH,
        )

    def send_lse(k):
        return pltpu.make_async_remote_copy(
            src_ref=lse_send.at[k // heads],
            dst_ref=lse_recv.at[me],
            send_sem=send_sem.at[1],
            recv_sem=recv_sem.at[1],
            device_id={"kv": k},
            device_id_type=MESH,
        )

    def send_att(k):
        mine = att.at[my_head * seqs + my_seq]
        return pltpu.make_async_remote_copy(
            src_ref=mine,
            dst_ref=mine,
            send_sem=send_sem.at[2],
            recv_sem=recv_sem.at[2],
            device_id={"kv": k},
            device_id_type=MESH,
        )

    def all_but_one(ref, n):
        some = ref.at[pl.ds(0, peers - 1)]
        return pltpu.make_async_remote_copy(
            src_ref=some,
            dst_ref=some,
            send_sem=send_sem.at[n],
            recv_sem=recv_sem.at[n],
            device_id={"kv": me},
            device_id_type=MESH,
        )

    planes = seqs // 2
    my_plane = my_seq // 2
    place = me * block + iota((1, block), 1)

    @pl.loop(0, planes // 2, init_carry=jnp.zeros((heads * props, 128), F32))
    def lse_cols(g, cols):
        members = []
        for far in (planes // 2 + g, planes // 2 - 1 - g):
            plane = (my_plane + far) % planes
            members += [2 * plane, 2 * plane + 1]
        for s in members:
            raw = dot_last(q_scr[s], kbuf[s])
            minus = jnp.where(place < lengths[s], -logcum[s], NEG_LARGE)
            cum = cum_scr[pl.ds(pl.multiple_of(s * props, props), props), :]
            scores = jnp.concatenate(
                [
                    raw[h * props : (h + 1) * props] * scaling
                    + (cum[:, h : h + 1] + minus[h : h + 1])
                    for h in range(heads)
                ],
                axis=0,
            )
            top = jnp.maximum(jnp.max(scores, axis=-1, keepdims=True), NEG_FLOOR)
            weights = jnp.exp(scores - top)
            total = jnp.sum(weights, axis=-1, keepdims=True)
            some = total > 0.0
            safe = jnp.where(some, total, 1.0)
            out = jnp.dot(weights.astype(BF16), vbuf[s], preferred_element_type=F32)
            out = (out * (1.0 / safe)).astype(BF16)
            o_send[pl.ds(s * heads, heads)] = out.reshape(heads, props, head)
            lse = jnp.where(some, top + jnp.log(safe), NEG_LARGE)
            cols = jnp.where(iota((heads * props, 128), 1) == s, lse, cols)
        for s in members:
            for h in range(heads):
                k = s * heads + h

                @pl.when(k != me)
                def _():
                    send_out(k).start()

                @pl.when(k == me)
                def _():
                    o_recv[me] = o_send[k]

        return cols

    padded = jnp.concatenate([lse_cols, jnp.zeros((128 - heads * props, 128), F32)], axis=0)
    lse_rows = padded.T
    for s in range(seqs):
        lse_send[s] = lse_rows[s : s + 1]
    lse_recv[me] = lse_send[my_seq]

    @pl.loop(1, peers)
    def _(step):
        send_lse((me + step) % peers).start()

    for name in ("accepted", "pending_keys", "pending_values"):
        loads[name].wait()
    width = heads * props
    q_own = q_scr[my_seq]
    own_rows = pl.ds(pl.multiple_of(my_seq * props, props), props)
    extra = 16
    pad = jnp.zeros((extra - taken, head), F32)
    keys_x = jnp.concatenate(
        [
            kn_scr[own_rows, :].astype(F32),
            pending_keys[my_seq].astype(F32),
            pad,
        ],
        axis=0,
    ).astype(BF16)
    values_x = jnp.concatenate(
        [
            vn_scr[own_rows, :].astype(F32),
            pending_values[my_seq].astype(F32),
            pad,
        ],
        axis=0,
    ).astype(BF16)
    raw_t = dot_last(keys_x, q_own)
    cum_own = cum_scr[own_rows, :]
    lane_head = iota((props, width), 1) // props
    lane_prop = iota((props, width), 1) & (props - 1)
    cum_wide = jnp.zeros((props, width), F32)
    for h in range(heads):
        cum_wide = jnp.where(lane_head == h, cum_own[:, h : h + 1], cum_wide)
    cum_row = jnp.sum(
        jnp.where(lane_prop == iota((props, width), 0), cum_wide, 0.0), axis=0, keepdims=True
    )
    anc_fold = (
        (iota((rows, width), 0) & (props - 1)) == (iota((rows, width), 1) & (props - 1))
    ).astype(BF16)
    anc_own = jnp.dot(anc_scr[own_rows, :], anc_fold, preferred_element_type=F32)
    pend_wide = jnp.zeros((extra, width), F32)
    pend_sub = iota((extra, width), 0)
    for a in range(taken):
        col = jnp.sum(
            jnp.where(iota((heads, seqs), 1) == my_seq, pending_logcum[a], 0.0),
            axis=1,
            keepdims=True,
        )
        row = jnp.sum(
            jnp.where(iota((heads, width), 1) // props == iota((heads, width), 0), col, 0.0),
            axis=0,
            keepdims=True,
        )
        pend_wide = jnp.where(pend_sub == a, row, pend_wide)
    tree_t = jnp.where(
        anc_own > 0.5, raw_t[:props] * scaling + cum_row - cum_wide, NEG_LARGE
    )
    pend_t = jnp.where(
        pend_sub < accepted[my_seq], raw_t[props:] * scaling + cum_row - pend_wide, NEG_LARGE
    )
    both_t = jnp.concatenate([tree_t, pend_t], axis=0)
    top_t = jnp.max(both_t, axis=0, keepdims=True)
    weights_t = jnp.exp(both_t - top_t)
    total_t = jnp.sum(weights_t, axis=0, keepdims=True)
    share_t = (weights_t * (1.0 / total_t)).astype(BF16)
    tree_scr[...] = lax.dot_general(
        share_t, values_x, (((0,), (0,)), ((), ())), preferred_element_type=F32
    )
    head_rows = pl.ds(pl.multiple_of(my_head * props, props), props)
    o_recv[peers] = tree_scr[head_rows, :].astype(BF16)
    lse_t = top_t + jnp.log(total_t)
    lse_recv[peers] = jnp.concatenate([lse_t, jnp.zeros((1, 128 - width), F32)], axis=1)

    all_but_one(lse_recv, 1).wait_recv()
    slots = peers + 8
    lse_all = lse_recv[:, 0, :]
    weight = jnp.exp(lse_all - jnp.max(lse_all, axis=0, keepdims=True)).astype(BF16)
    pick = (
        (iota((128, 128), 0) - my_head * props) == (iota((128, 128), 1) & (props - 1))
    ).astype(BF16)
    picked = jnp.dot(weight, pick, preferred_element_type=F32)
    mine_8 = iota((8, 128), 1) // props == iota((8, 128), 0)
    mine_16 = (iota((props, 128), 1) & (props - 1)) == iota((props, 128), 0)
    mixes = []
    for c in range(slots // 8):
        flat = jnp.sum(
            jnp.where(mine_8, picked[c * 8 : (c + 1) * 8], 0.0), axis=0, keepdims=True
        )
        mixes.append(jnp.where(mine_16, flat, 0.0))
    den = functools.reduce(lambda a, b: a + b, mixes)
    den = jnp.sum(den, axis=1, keepdims=True)
    mix = jnp.concatenate(mixes, axis=1).astype(BF16)
    all_but_one(o_recv, 0).wait_recv()
    blended = jnp.dot(
        mix, o_recv[...].reshape(slots * props, head), preferred_element_type=F32
    )
    att[my_head * seqs + my_seq] = (blended / den).astype(BF16)

    @pl.loop(1, peers)
    def _(step):
        send_att((me + step) % peers).start()

    all_but_one(att, 2).wait_recv()

    loads["out_weight"].wait()
    part_t = jnp.zeros((out_weight.shape[0], rows), F32)
    for h in range(heads):
        part_t += dot_last(
            out_weight[:, h * head : (h + 1) * head],
            att[pl.ds(h * seqs, seqs)].reshape(rows, head),
        )
    half = out_weight.shape[0] // 2
    low, high = part_t[:half].astype(BF16), part_t[half:].astype(BF16)
    swap_send[...] = jnp.where(core == 0, high, low)
    swap = pltpu.make_async_remote_copy(
        src_ref=swap_send,
        dst_ref=swap_recv,
        send_sem=send_sem.at[3],
        recv_sem=recv_sem.at[3],
        device_id={"tp": 1 - core},
        device_id_type=MESH,
    )
    swap.start()
    kept = jnp.where(core == 0, low, high).astype(F32)
    swap.wait()
    final = kept + swap_recv[...].astype(F32)
    result[...] = final.T.astype(BF16).reshape(seqs, props, half)

    all_but_one(o_send, 0).wait_send()
    all_but_one(lse_recv, 1).wait_send()
    all_but_one(att, 2).wait_send()


def shards(
    tokens,
    norm_gain,
    query_weight,
    key_weight,
    value_weight,
    forget_weight,
    forget_bias,
    query_gain,
    key_gain,
    output_weight,
    cache_keys,
    cache_values,
    cache_logcum,
    pending_keys,
    pending_values,
    pending_logcum,
    lengths,
    accepted,
    parents,
):
    seqs, props, width = tokens.shape
    head = query_gain.shape[0]
    heads = query_weight.shape[1] // head
    block = cache_keys.shape[1]
    taken = pending_keys.shape[1]
    rows = seqs * props
    peers = seqs * heads
    half = output_weight.shape[1] // 2
    operands = {
        "tokens": tokens.reshape(rows, width),
        "norm_gain": norm_gain.reshape(1, width),
        "query_weight": query_weight,
        "key_weight": key_weight,
        "value_weight": value_weight,
        "forget": forget_weight.T,
        "forget_bias": forget_bias,
        "query_gain": query_gain.reshape(1, head),
        "key_gain": key_gain.reshape(1, head),
        "out_weight": output_weight.T,
        "keys": cache_keys.reshape(seqs, block, head),
        "values": cache_values.reshape(seqs, block, head),
        "logcum": jnp.swapaxes(cache_logcum, 1, 2),
        "pending_keys": pending_keys.reshape(seqs, taken, head),
        "pending_values": pending_values.reshape(seqs, taken, head),
        "pending_logcum": jnp.transpose(pending_logcum, (1, 2, 0)),
        "lengths": lengths,
        "accepted": accepted,
        "accepted_row": accepted.reshape(1, seqs),
        "parents": parents,
    }
    places = {
        name: (pltpu.SMEM if name in SCALARS else pltpu.VMEM)(array.shape, array.dtype)
        for name, array in operands.items()
    }
    return pl.pallas_call(
        functools.partial(kernel, seqs, heads, props, head, taken, block),
        out_shape=jax.ShapeDtypeStruct((seqs, props, half), BF16),
        in_specs=[{name: pl.BlockSpec(memory_space=pltpu.HBM) for name in operands}],
        out_specs=pl.BlockSpec(memory_space=pltpu.VMEM),
        scratch_shapes=[
            places,
            pltpu.VMEM((rows, width), BF16),
            pltpu.VMEM((seqs, heads * props, head), BF16),
            pltpu.VMEM((rows, head), BF16),
            pltpu.VMEM((rows, head), BF16),
            pltpu.VMEM((rows, rows), BF16),
            pltpu.VMEM((rows, 2 * heads), F32),
            pltpu.VMEM((peers, props, head), BF16),
            pltpu.VMEM((peers + 8, props, head), BF16),
            pltpu.VMEM((seqs, 1, 128), F32),
            pltpu.VMEM((peers + 8, 1, 128), F32),
            pltpu.VMEM((heads * props, head), F32),
            pltpu.VMEM((peers, props, head), BF16),
            pltpu.VMEM((half, rows), BF16),
            pltpu.VMEM((half, rows), BF16),
            pltpu.SemaphoreType.DMA((len(operands),)),
            pltpu.SemaphoreType.DMA((4,)),
            pltpu.SemaphoreType.DMA((4,)),
        ],
        compiler_params=pltpu.CompilerParams(
            collective_id=0, has_side_effects=True, vmem_limit_bytes=67043328
        ),
    )(operands)


def solution(mesh):
    placed = (
        P("dp", None, None),
        P(),
        P(None, "tp"),
        P(None, "tp"),
        P(None, "tp"),
        P(),
        P(),
        P(),
        P(),
        P("tp", "kv"),
        P("dp", "kv", "tp", None),
        P("dp", "kv", "tp", None),
        P("dp", "kv", "tp"),
        P("dp", None, "tp", None),
        P("dp", None, "tp", None),
        P("dp", None, "tp"),
        P("dp"),
        P("dp"),
        P("dp", None),
    )
    return jax.shard_map(
        shards, mesh=mesh, in_specs=placed, out_specs=P("dp", None, ("kv", "tp")), check_vma=False
    )
```

```python
import functools

import jax
import jax.numpy as jnp
from jax import lax
from jax.experimental import pallas as pl
from jax.experimental.pallas import tpu as pltpu
from jax.sharding import PartitionSpec as P

EPSILON = 1e-06
NEG_LARGE = -1e30
NEG_FLOOR = -1e29
ROUNDS = 2
HIGHEST = lax.Precision.HIGHEST
MESH = pl.DeviceIdType.MESH
F32 = jnp.float32
BF16 = jnp.bfloat16
LAST = (((1,), (1,)), ((), ()))
NAMES = (
    "tokens",
    "norm_gain",
    "query_weight",
    "key_weight",
    "value_weight",
    "forget",
    "forget_bias",
    "query_gain",
    "key_gain",
    "out_weight",
    "keys",
    "values",
    "logcum",
    "pending_keys",
    "pending_values",
    "pending_logcum",
    "lengths",
    "accepted",
    "accepted_row",
    "parents",
)
SCALARS = ("forget_bias", "lengths", "accepted")
LOAD_ORDER = (
    "parents",
    "tokens",
    "norm_gain",
    "forget",
    "forget_bias",
    "accepted_row",
    "pending_logcum",
    "key_gain",
    "query_gain",
    "key_weight",
    "value_weight",
    "query_weight",
    "keys",
    "logcum",
    "lengths",
    "values",
    "accepted",
    "pending_keys",
    "pending_values",
    "out_weight",
)


def iota(shape, dim):
    return lax.broadcasted_iota(jnp.int32, shape, dim)


def dot_last(a, b):
    return lax.dot_general(a, b, LAST, preferred_element_type=F32)


def by_distance(count):
    return sorted(range(count), key=lambda d: -min(d, count - d))


def unit(rows, gain):
    return rows * lax.rsqrt(jnp.mean(rows * rows, axis=-1, keepdims=True) + EPSILON) * gain


def kernel(
    seqs,
    heads,
    props,
    head,
    taken,
    block,
    operands,
    result,
    places,
    normed,
    scale_scr,
    q_scr,
    kn_scr,
    vn_scr,
    anc_scr,
    cum_scr,
    o_send,
    o_recv,
    lse_send,
    lse_recv,
    tree_scr,
    att,
    swap_send,
    swap_recv,
    load_sem,
    send_sem,
    recv_sem,
):
    rows = seqs * props
    peers = seqs * heads
    scaling = head**-0.5
    me = lax.axis_index("kv")
    core = lax.axis_index("tp")
    across_y = 2 * heads
    planes = seqs // 2
    my_z = me // across_y
    my_y = me & (across_y - 1)
    my_seq = me // heads
    my_head = me & (heads - 1)
    z_at = [((my_z + dz) & (planes - 1)) * across_y for dz in range(planes)]
    y_at = [(my_y + dy) & (across_y - 1) for dy in range(across_y)]
    others = sorted(
        ((dz, dy) for dz in range(planes) for dy in range(across_y) if dz or dy),
        key=lambda d: -min(d[0], planes - d[0]) - min(d[1], across_y - d[1]),
    )

    wkv = places["key_weight"]
    places = dict(
        places, key_weight=wkv.at[:, pl.ds(0, head)], value_weight=wkv.at[:, pl.ds(head, head)]
    )
    loads = {
        name: pltpu.make_async_copy(operands[name], places[name], load_sem.at[n])
        for n, name in enumerate(LOAD_ORDER)
    }
    for item in loads.values():
        item.start()
    (
        tok, norm_gain, wq, _, _, forget, forget_bias, query_gain, key_gain, out_weight,
        kbuf, vbuf, logcum, pending_keys, pending_values, pending_logcum, lengths, accepted,
        accepted_row, parents,
    ) = (places[name] for name in NAMES)

    barrier = pltpu.get_barrier_semaphore()

    for dz, dy in others:
        pl.semaphore_signal(
            barrier, inc=1, device_id={"kv": z_at[dz] + y_at[dy]}, device_id_type=MESH
        )
    pl.semaphore_signal(barrier, inc=1, device_id={"tp": 1 - core}, device_id_type=MESH)

    loads["parents"].wait()

    lane = iota((seqs, rows), 1)
    spread = ((iota((props, rows), 1) & (props - 1)) == iota((props, rows), 0)).astype(BF16)
    repeated = jnp.dot(
        parents[...].astype(F32).astype(BF16), spread, preferred_element_type=F32
    )
    parent_row = jnp.sum(
        jnp.where(lane // props == iota((seqs, rows), 0), repeated, 0.0), axis=0, keepdims=True
    ).astype(jnp.int32)
    down = iota((rows, rows), 0)
    across = iota((rows, rows), 1)
    same = down // props == across // props
    linked = (same & (parent_row == (down & (props - 1)))) | (down == across)
    anc_t = jnp.where(linked, 1.0, 0.0).astype(BF16)
    for _ in range((props - 1).bit_length()):
        anc_t = jnp.minimum(jnp.dot(anc_t, anc_t, preferred_element_type=F32), 1.0).astype(BF16)
    anc_scr[...] = anc_t

    loads["tokens"].wait()
    loads["norm_gain"].wait()

    model = tok.shape[1]

    @pl.loop(0, rows // 32)
    def _(step):
        piece = pl.ds(step * 32, 32)
        total = jnp.zeros((32, 128), F32)
        for c in range(model // 128):
            wide = tok[piece, c * 128 : (c + 1) * 128].astype(F32)
            total += wide * wide
        scale_scr[piece, :] = total

    mean = jnp.sum(scale_scr[...], axis=1, keepdims=True) * (1.0 / model)
    scale_scr[...] = jnp.broadcast_to(lax.rsqrt(mean + EPSILON), (rows, 128))

    @pl.loop(0, rows // 32)
    def _(step):
        piece = pl.ds(step * 32, 32)
        scale = scale_scr[piece, :]
        for c in range(model // 128):
            columns = slice(c * 128, (c + 1) * 128)
            wide = tok[piece, columns].astype(F32)
            normed[piece, columns] = (wide * scale * norm_gain[:, columns]).astype(BF16)

    for name in (
        "forget", "forget_bias", "accepted_row", "pending_logcum", "key_gain", "query_gain",
        "key_weight", "value_weight", "query_weight",
    ):
        loads[name].wait()
    gate_raw = dot_last(forget[...], normed[...])
    gate_head = iota((2 * heads, 1), 0)
    bias = jnp.zeros((2 * heads, 1), F32)
    for n in range(2 * heads):
        bias = jnp.where(gate_head == n, forget_bias[n], bias)
    gate_raw = gate_raw + bias
    gates = jnp.minimum(gate_raw, 0.0) - jnp.log1p(jnp.exp(-jnp.abs(gate_raw)))
    gates = jnp.where(
        core == 0, gates, jnp.concatenate([gates[heads:], gates[:heads]], axis=0)
    )
    base = jnp.zeros((heads, seqs), F32)
    for a in range(taken):
        base = jnp.where(accepted_row[...] - 1 == a, pending_logcum[a], base)
    base = jnp.concatenate([base, jnp.zeros((heads, seqs), F32)], axis=0)
    expand = (lane // props == iota((seqs, rows), 0)).astype(F32)
    cum_t = jnp.dot(
        gates, anc_t.astype(F32), precision=HIGHEST, preferred_element_type=F32
    ) + jnp.dot(base, expand, precision=HIGHEST, preferred_element_type=F32)
    cum_scr[...] = cum_t.T

    sides = jnp.dot(normed[...], wkv[...], preferred_element_type=F32)
    kn_scr[...] = unit(sides[:, :head], key_gain[...]).astype(BF16)
    vn_scr[...] = sides[:, head:].astype(BF16)
    for pair in range(heads // 2):
        raw = jnp.dot(
            normed[...],
            wq[:, 2 * pair * head : (2 * pair + 2) * head],
            preferred_element_type=F32,
        )
        for h in (2 * pair, 2 * pair + 1):
            one = raw[:, (h - 2 * pair) * head : (h - 2 * pair + 1) * head]
            q_scr[:, h * props : (h + 1) * props, :] = (
                unit(one, query_gain[...]).astype(BF16).reshape(seqs, props, head)
            )

    o_recv[pl.ds(peers, 8)] = jnp.zeros((8, props, head), BF16)
    lse_recv[pl.ds(peers, 8)] = jnp.full((8, 1, 128), NEG_LARGE, F32)

    for name in ("keys", "logcum", "lengths", "values"):
        loads[name].wait()
    def send_out(k):
        return pltpu.make_async_remote_copy(
            src_ref=o_send.at[k],
            dst_ref=o_recv.at[me],
            send_sem=send_sem.at[0],
            recv_sem=recv_sem.at[0],
            device_id={"kv": k},
            device_id_type=MESH,
        )

    def send_lse(k):
        return pltpu.make_async_remote_copy(
            src_ref=lse_send.at[lax.shift_right_logical(k, heads.bit_length() - 1)],
            dst_ref=lse_recv.at[me],
            send_sem=send_sem.at[1],
            recv_sem=recv_sem.at[1],
            device_id={"kv": k},
            device_id_type=MESH,
        )

    def send_att(k):
        mine = att.at[my_head * seqs + my_seq]
        return pltpu.make_async_remote_copy(
            src_ref=mine,
            dst_ref=mine,
            send_sem=send_sem.at[2],
            recv_sem=recv_sem.at[2],
            device_id={"kv": k},
            device_id_type=MESH,
        )

    def all_but_one(ref, n):
        some = ref.at[pl.ds(0, peers - 1)]
        return pltpu.make_async_remote_copy(
            src_ref=some,
            dst_ref=some,
            send_sem=send_sem.at[n],
            recv_sem=recv_sem.at[n],
            device_id={"kv": me},
            device_id_type=MESH,
        )

    place = me * block + iota((1, block), 1)
    slot = iota((heads * props, 128), 1)
    far_first = by_distance(planes)
    for g in range(ROUNDS):
        fars = far_first[g * planes // ROUNDS : (g + 1) * planes // ROUNDS]
        members = [lax.shift_right_logical(z_at[far], heads.bit_length() - 1) + half for far in fars for half in range(2)]
        cols = jnp.zeros((heads * props, 128), F32)
        for j, s in enumerate(members):
            raw = dot_last(q_scr[s], kbuf[s])
            minus = jnp.where(place < lengths[s], -logcum[s], NEG_LARGE)
            cum = cum_scr[pl.ds(pl.multiple_of(s * props, props), props), :]
            scores = jnp.concatenate(
                [
                    raw[h * props : (h + 1) * props] * scaling
                    + (cum[:, h : h + 1] + minus[h : h + 1])
                    for h in range(heads)
                ],
                axis=0,
            )
            top = jnp.maximum(jnp.max(scores, axis=-1, keepdims=True), NEG_FLOOR)
            weights = jnp.exp(scores - top)
            total = jnp.sum(weights, axis=-1, keepdims=True)
            some = total > 0.0
            safe = jnp.where(some, total, 1.0)
            out = jnp.dot(weights.astype(BF16), vbuf[s], preferred_element_type=F32)
            out = (out * (1.0 / safe)).astype(BF16)
            o_send[pl.ds(s * heads, heads)] = out.reshape(heads, props, head)
            lse = jnp.where(some, top + jnp.log(safe), NEG_LARGE)
            cols = jnp.where(slot == j, lse, cols)
        lse_rows = jnp.concatenate(
            [cols, jnp.zeros((128 - heads * props, 128), F32)], axis=0
        ).T
        for j, s in enumerate(members):
            lse_send[s] = lse_rows[j : j + 1]
        if g == 0:
            pl.semaphore_wait(barrier, peers)
        for far in fars:
            for dy in by_distance(across_y):
                if far or dy:
                    send_out(z_at[far] + y_at[dy]).start()
                    send_lse(z_at[far] + y_at[dy]).start()

    o_recv[me] = o_send[me]
    lse_recv[me] = lse_send[my_seq]

    for name in ("accepted", "pending_keys", "pending_values"):
        loads[name].wait()
    width = heads * props
    q_own = q_scr[my_seq]
    own_rows = pl.ds(pl.multiple_of(my_seq * props, props), props)
    extra = 16
    pad = jnp.zeros((extra - taken, head), F32)
    keys_x = jnp.concatenate(
        [
            kn_scr[own_rows, :].astype(F32),
            pending_keys[my_seq].astype(F32),
            pad,
        ],
        axis=0,
    ).astype(BF16)
    values_x = jnp.concatenate(
        [
            vn_scr[own_rows, :].astype(F32),
            pending_values[my_seq].astype(F32),
            pad,
        ],
        axis=0,
    ).astype(BF16)
    raw_t = dot_last(keys_x, q_own)
    cum_own = cum_scr[own_rows, :]
    lane_head = iota((props, width), 1) // props
    lane_prop = iota((props, width), 1) & (props - 1)
    cum_wide = jnp.zeros((props, width), F32)
    for h in range(heads):
        cum_wide = jnp.where(lane_head == h, cum_own[:, h : h + 1], cum_wide)
    cum_row = jnp.sum(
        jnp.where(lane_prop == iota((props, width), 0), cum_wide, 0.0), axis=0, keepdims=True
    )
    anc_fold = (
        (iota((rows, width), 0) & (props - 1)) == (iota((rows, width), 1) & (props - 1))
    ).astype(BF16)
    anc_own = jnp.dot(anc_scr[own_rows, :], anc_fold, preferred_element_type=F32)
    pend_wide = jnp.zeros((extra, width), F32)
    pend_sub = iota((extra, width), 0)
    for a in range(taken):
        col = jnp.sum(
            jnp.where(iota((heads, seqs), 1) == my_seq, pending_logcum[a], 0.0),
            axis=1,
            keepdims=True,
        )
        row = jnp.sum(
            jnp.where(iota((heads, width), 1) // props == iota((heads, width), 0), col, 0.0),
            axis=0,
            keepdims=True,
        )
        pend_wide = jnp.where(pend_sub == a, row, pend_wide)
    tree_t = jnp.where(
        anc_own > 0.5, raw_t[:props] * scaling + cum_row - cum_wide, NEG_LARGE
    )
    pend_t = jnp.where(
        pend_sub < accepted[my_seq], raw_t[props:] * scaling + cum_row - pend_wide, NEG_LARGE
    )
    both_t = jnp.concatenate([tree_t, pend_t], axis=0)
    top_t = jnp.max(both_t, axis=0, keepdims=True)
    weights_t = jnp.exp(both_t - top_t)
    total_t = jnp.sum(weights_t, axis=0, keepdims=True)
    share_t = (weights_t * (1.0 / total_t)).astype(BF16)
    tree_scr[...] = lax.dot_general(
        share_t, values_x, (((0,), (0,)), ((), ())), preferred_element_type=F32
    )
    head_rows = pl.ds(pl.multiple_of(my_head * props, props), props)
    o_recv[peers] = tree_scr[head_rows, :].astype(BF16)
    lse_t = top_t + jnp.log(total_t)
    lse_recv[peers] = jnp.concatenate([lse_t, jnp.zeros((1, 128 - width), F32)], axis=1)

    all_but_one(lse_recv, 1).wait_recv()
    slots = peers + 8
    lse_all = lse_recv[:, 0, :]
    weight = jnp.exp(lse_all - jnp.max(lse_all, axis=0, keepdims=True)).astype(BF16)
    pick = (
        (iota((128, 128), 0) - my_head * props) == (iota((128, 128), 1) & (props - 1))
    ).astype(BF16)
    picked = jnp.dot(weight, pick, preferred_element_type=F32)
    mine_8 = iota((8, 128), 1) // props == iota((8, 128), 0)
    mine_16 = (iota((props, 128), 1) & (props - 1)) == iota((props, 128), 0)
    mixes = []
    for c in range(slots // 8):
        flat = jnp.sum(
            jnp.where(mine_8, picked[c * 8 : (c + 1) * 8], 0.0), axis=0, keepdims=True
        )
        mixes.append(jnp.where(mine_16, flat, 0.0))
    den = functools.reduce(lambda a, b: a + b, mixes)
    den = jnp.sum(den, axis=1, keepdims=True)
    mix = jnp.concatenate(mixes, axis=1).astype(BF16)
    all_but_one(o_recv, 0).wait_recv()
    blended = jnp.dot(
        mix, o_recv[...].reshape(slots * props, head), preferred_element_type=F32
    )
    att[my_head * seqs + my_seq] = (blended / den).astype(BF16)

    for dz, dy in others:
        send_att(z_at[dz] + y_at[dy]).start()

    all_but_one(att, 2).wait_recv()

    loads["out_weight"].wait()
    part_t = jnp.zeros((out_weight.shape[0], rows), F32)
    for h in range(heads):
        part_t += dot_last(
            out_weight[:, h * head : (h + 1) * head],
            att[pl.ds(h * seqs, seqs)].reshape(rows, head),
        )
    half = out_weight.shape[0] // 2
    low, high = part_t[:half].astype(BF16), part_t[half:].astype(BF16)
    swap_send[...] = jnp.where(core == 0, high, low)
    swap = pltpu.make_async_remote_copy(
        src_ref=swap_send,
        dst_ref=swap_recv,
        send_sem=send_sem.at[3],
        recv_sem=recv_sem.at[3],
        device_id={"tp": 1 - core},
        device_id_type=MESH,
    )
    swap.start()
    kept = jnp.where(core == 0, low, high).astype(F32)
    swap.wait()
    final = kept + swap_recv[...].astype(F32)
    result[...] = final.T.astype(BF16).reshape(seqs, props, half)

    all_but_one(o_send, 0).wait_send()
    all_but_one(lse_recv, 1).wait_send()
    all_but_one(att, 2).wait_send()


def shards(
    tokens,
    norm_gain,
    query_weight,
    key_weight,
    value_weight,
    forget_weight,
    forget_bias,
    query_gain,
    key_gain,
    output_weight,
    cache_keys,
    cache_values,
    cache_logcum,
    pending_keys,
    pending_values,
    pending_logcum,
    lengths,
    accepted,
    parents,
):
    seqs, props, width = tokens.shape
    head = query_gain.shape[0]
    heads = query_weight.shape[1] // head
    block = cache_keys.shape[1]
    taken = pending_keys.shape[1]
    rows = seqs * props
    peers = seqs * heads
    half = output_weight.shape[1] // 2
    operands = {
        "tokens": tokens.reshape(rows, width),
        "norm_gain": norm_gain.reshape(1, width),
        "query_weight": query_weight,
        "key_weight": key_weight,
        "value_weight": value_weight,
        "forget": forget_weight.T,
        "forget_bias": forget_bias,
        "query_gain": query_gain.reshape(1, head),
        "key_gain": key_gain.reshape(1, head),
        "out_weight": output_weight.T,
        "keys": cache_keys.reshape(seqs, block, head),
        "values": cache_values.reshape(seqs, block, head),
        "logcum": jnp.swapaxes(cache_logcum, 1, 2),
        "pending_keys": pending_keys.reshape(seqs, taken, head),
        "pending_values": pending_values.reshape(seqs, taken, head),
        "pending_logcum": jnp.transpose(pending_logcum, (1, 2, 0)),
        "lengths": lengths,
        "accepted": accepted,
        "accepted_row": accepted.reshape(1, seqs),
        "parents": parents,
    }
    places = {
        name: (pltpu.SMEM if name in SCALARS else pltpu.VMEM)(array.shape, array.dtype)
        for name, array in operands.items()
        if name != "value_weight"
    }
    places["key_weight"] = pltpu.VMEM((width, 2 * head), BF16)
    return pl.pallas_call(
        functools.partial(kernel, seqs, heads, props, head, taken, block),
        out_shape=jax.ShapeDtypeStruct((seqs, props, half), BF16),
        in_specs=[{name: pl.BlockSpec(memory_space=pltpu.HBM) for name in operands}],
        out_specs=pl.BlockSpec(memory_space=pltpu.VMEM),
        scratch_shapes=[
            places,
            pltpu.VMEM((rows, width), BF16),
            pltpu.VMEM((rows, 128), F32),
            pltpu.VMEM((seqs, heads * props, head), BF16),
            pltpu.VMEM((rows, head), BF16),
            pltpu.VMEM((rows, head), BF16),
            pltpu.VMEM((rows, rows), BF16),
            pltpu.VMEM((rows, 2 * heads), F32),
            pltpu.VMEM((peers, props, head), BF16),
            pltpu.VMEM((peers + 8, props, head), BF16),
            pltpu.VMEM((seqs, 1, 128), F32),
            pltpu.VMEM((peers + 8, 1, 128), F32),
            pltpu.VMEM((heads * props, head), F32),
            pltpu.VMEM((peers, props, head), BF16),
            pltpu.VMEM((half, rows), BF16),
            pltpu.VMEM((half, rows), BF16),
            pltpu.SemaphoreType.DMA((len(operands),)),
            pltpu.SemaphoreType.DMA((4,)),
            pltpu.SemaphoreType.DMA((4,)),
        ],
        compiler_params=pltpu.CompilerParams(
            collective_id=0, has_side_effects=True, vmem_limit_bytes=67043328
        ),
    )(operands)


def solution(mesh):
    placed = (
        P("dp", None, None),
        P(),
        P(None, "tp"),
        P(None, "tp"),
        P(None, "tp"),
        P(),
        P(),
        P(),
        P(),
        P("tp", "kv"),
        P("dp", "kv", "tp", None),
        P("dp", "kv", "tp", None),
        P("dp", "kv", "tp"),
        P("dp", None, "tp", None),
        P("dp", None, "tp", None),
        P("dp", None, "tp"),
        P("dp"),
        P("dp"),
        P("dp", None),
    )
    return jax.shard_map(
        shards, mesh=mesh, in_specs=placed, out_specs=P("dp", None, ("kv", "tp")), check_vma=False
    )
```

```python
import functools

import jax
import jax.numpy as jnp
from jax import lax
from jax.experimental import pallas as pl
from jax.experimental.pallas import tpu as pltpu
from jax.sharding import PartitionSpec as P

EPSILON = 1e-06
NEG_LARGE = -1e30
NEG_FLOOR = -1e29
ROUNDS = (2, 2, 4)
HIGHEST = lax.Precision.HIGHEST
MESH = pl.DeviceIdType.MESH
F32 = jnp.float32
BF16 = jnp.bfloat16
LAST = (((1,), (1,)), ((), ()))
NAMES = (
    "tokens",
    "norm_gain",
    "query_weight",
    "key_weight",
    "value_weight",
    "forget",
    "forget_bias",
    "query_gain",
    "key_gain",
    "out_weight",
    "keys",
    "values",
    "logcum",
    "pending_keys",
    "pending_values",
    "pending_logcum",
    "lengths",
    "accepted",
    "accepted_row",
    "parents",
)
SCALARS = ("forget_bias", "lengths", "accepted")
LOAD_ORDER = (
    "parents",
    "tokens",
    "norm_gain",
    "forget",
    "forget_bias",
    "accepted_row",
    "pending_logcum",
    "key_gain",
    "query_gain",
    "key_weight",
    "value_weight",
    "query_weight",
    "keys",
    "logcum",
    "lengths",
    "values",
    "accepted",
    "pending_keys",
    "pending_values",
    "out_weight",
)


def iota(shape, dim):
    return lax.broadcasted_iota(jnp.int32, shape, dim)


def dot_last(a, b):
    return lax.dot_general(a, b, LAST, preferred_element_type=F32)


def by_distance(count):
    return sorted(range(count), key=lambda d: -min(d, count - d))


def unit(rows, gain):
    return rows * lax.rsqrt(jnp.mean(rows * rows, axis=-1, keepdims=True) + EPSILON) * gain


def kernel(
    seqs,
    heads,
    props,
    head,
    taken,
    block,
    operands,
    result,
    places,
    normed,
    scale_scr,
    q_scr,
    kn_scr,
    vn_scr,
    anc_scr,
    cum_scr,
    o_send,
    o_recv,
    lse_send,
    lse_recv,
    tree_scr,
    att,
    swap_send,
    swap_recv,
    load_sem,
    send_sem,
    recv_sem,
):
    rows = seqs * props
    peers = seqs * heads
    scaling = head**-0.5
    me = lax.axis_index("kv")
    core = lax.axis_index("tp")
    across_y = 2 * heads
    planes = seqs // 2
    my_z = me // across_y
    my_y = me & (across_y - 1)
    my_seq = me // heads
    my_head = me & (heads - 1)
    z_at = [((my_z + dz) & (planes - 1)) * across_y for dz in range(planes)]
    y_at = [(my_y + dy) & (across_y - 1) for dy in range(across_y)]
    others = sorted(
        ((dz, dy) for dz in range(planes) for dy in range(across_y) if dz or dy),
        key=lambda d: -min(d[0], planes - d[0]) - min(d[1], across_y - d[1]),
    )

    wkv = places["key_weight"]
    places = dict(
        places, key_weight=wkv.at[:, pl.ds(0, head)], value_weight=wkv.at[:, pl.ds(head, head)]
    )
    loads = {
        name: pltpu.make_async_copy(operands[name], places[name], load_sem.at[n])
        for n, name in enumerate(LOAD_ORDER)
    }
    for item in loads.values():
        item.start()
    (
        tok, norm_gain, wq, _, _, forget, forget_bias, query_gain, key_gain, out_weight,
        kbuf, vbuf, logcum, pending_keys, pending_values, pending_logcum, lengths, accepted,
        accepted_row, parents,
    ) = (places[name] for name in NAMES)

    barrier = pltpu.get_barrier_semaphore()

    for dz, dy in others:
        pl.semaphore_signal(
            barrier, inc=1, device_id={"kv": z_at[dz] + y_at[dy]}, device_id_type=MESH
        )
    pl.semaphore_signal(barrier, inc=1, device_id={"tp": 1 - core}, device_id_type=MESH)

    loads["parents"].wait()

    lane = iota((seqs, rows), 1)
    spread = ((iota((props, rows), 1) & (props - 1)) == iota((props, rows), 0)).astype(BF16)
    repeated = jnp.dot(
        parents[...].astype(F32).astype(BF16), spread, preferred_element_type=F32
    )
    parent_row = jnp.sum(
        jnp.where(lane // props == iota((seqs, rows), 0), repeated, 0.0), axis=0, keepdims=True
    ).astype(jnp.int32)
    down = iota((rows, rows), 0)
    across = iota((rows, rows), 1)
    same = down // props == across // props
    linked = (same & (parent_row == (down & (props - 1)))) | (down == across)
    anc_t = jnp.where(linked, 1.0, 0.0).astype(BF16)
    for _ in range((props - 1).bit_length()):
        anc_t = jnp.minimum(jnp.dot(anc_t, anc_t, preferred_element_type=F32), 1.0).astype(BF16)
    anc_scr[...] = anc_t

    loads["tokens"].wait()
    loads["norm_gain"].wait()

    model = tok.shape[1]

    @pl.loop(0, rows // 32)
    def _(step):
        piece = pl.ds(step * 32, 32)
        total = jnp.zeros((32, 128), F32)
        for c in range(model // 128):
            wide = tok[piece, c * 128 : (c + 1) * 128].astype(F32)
            total += wide * wide
        scale_scr[piece, :] = total

    mean = jnp.sum(scale_scr[...], axis=1, keepdims=True) * (1.0 / model)
    scale_scr[...] = jnp.broadcast_to(lax.rsqrt(mean + EPSILON), (rows, 128))

    @pl.loop(0, rows // 32)
    def _(step):
        piece = pl.ds(step * 32, 32)
        scale = scale_scr[piece, :]
        for c in range(model // 128):
            columns = slice(c * 128, (c + 1) * 128)
            wide = tok[piece, columns].astype(F32)
            normed[piece, columns] = (wide * scale * norm_gain[:, columns]).astype(BF16)

    for name in (
        "forget", "forget_bias", "accepted_row", "pending_logcum", "key_gain", "query_gain",
        "key_weight", "value_weight", "query_weight",
    ):
        loads[name].wait()
    gate_raw = dot_last(forget[...], normed[...])
    gate_head = iota((2 * heads, 1), 0)
    bias = jnp.zeros((2 * heads, 1), F32)
    for n in range(2 * heads):
        bias = jnp.where(gate_head == n, forget_bias[n], bias)
    gate_raw = gate_raw + bias
    gates = jnp.minimum(gate_raw, 0.0) - jnp.log1p(jnp.exp(-jnp.abs(gate_raw)))
    gates = jnp.where(
        core == 0, gates, jnp.concatenate([gates[heads:], gates[:heads]], axis=0)
    )
    base = jnp.zeros((heads, seqs), F32)
    for a in range(taken):
        base = jnp.where(accepted_row[...] - 1 == a, pending_logcum[a], base)
    base = jnp.concatenate([base, jnp.zeros((heads, seqs), F32)], axis=0)
    expand = (lane // props == iota((seqs, rows), 0)).astype(F32)
    cum_t = jnp.dot(
        gates, anc_t.astype(F32), precision=HIGHEST, preferred_element_type=F32
    ) + jnp.dot(base, expand, precision=HIGHEST, preferred_element_type=F32)
    cum_scr[...] = cum_t.T

    sides = jnp.dot(normed[...], wkv[...], preferred_element_type=F32)
    kn_scr[...] = unit(sides[:, :head], key_gain[...]).astype(BF16)
    vn_scr[...] = sides[:, head:].astype(BF16)
    for pair in range(heads // 2):
        raw = jnp.dot(
            normed[...],
            wq[:, 2 * pair * head : (2 * pair + 2) * head],
            preferred_element_type=F32,
        )
        for h in (2 * pair, 2 * pair + 1):
            one = raw[:, (h - 2 * pair) * head : (h - 2 * pair + 1) * head]
            q_scr[:, h * props : (h + 1) * props, :] = (
                unit(one, query_gain[...]).astype(BF16).reshape(seqs, props, head)
            )

    o_recv[pl.ds(peers, 8)] = jnp.zeros((8, props, head), BF16)
    lse_recv[pl.ds(peers, 8)] = jnp.full((8, 1, 128), NEG_LARGE, F32)

    for name in ("keys", "logcum", "lengths", "values"):
        loads[name].wait()
    def send_out(k):
        return pltpu.make_async_remote_copy(
            src_ref=o_send.at[k],
            dst_ref=o_recv.at[me],
            send_sem=send_sem.at[0],
            recv_sem=recv_sem.at[0],
            device_id={"kv": k},
            device_id_type=MESH,
        )

    def send_lse(k):
        return pltpu.make_async_remote_copy(
            src_ref=lse_send.at[lax.shift_right_logical(k, heads.bit_length() - 1)],
            dst_ref=lse_recv.at[me],
            send_sem=send_sem.at[1],
            recv_sem=recv_sem.at[1],
            device_id={"kv": k},
            device_id_type=MESH,
        )

    def send_att(k):
        mine = att.at[my_head * seqs + my_seq]
        return pltpu.make_async_remote_copy(
            src_ref=mine,
            dst_ref=mine,
            send_sem=send_sem.at[2],
            recv_sem=recv_sem.at[2],
            device_id={"kv": k},
            device_id_type=MESH,
        )

    def all_but_one(ref, n):
        some = ref.at[pl.ds(0, peers - 1)]
        return pltpu.make_async_remote_copy(
            src_ref=some,
            dst_ref=some,
            send_sem=send_sem.at[n],
            recv_sem=recv_sem.at[n],
            device_id={"kv": me},
            device_id_type=MESH,
        )

    def send_planes(fars):
        for far in fars:
            for dy in by_distance(across_y):
                if far or dy:
                    send_out(z_at[far] + y_at[dy]).start()
                    send_lse(z_at[far] + y_at[dy]).start()

    place = me * block + iota((1, block), 1)
    slot = iota((heads * props, 128), 1)
    late = my_z >= planes // 2
    far_first = by_distance(planes)
    for g in range(len(ROUNDS)):
        fars = far_first[sum(ROUNDS[:g]) * planes // 8 : sum(ROUNDS[: g + 1]) * planes // 8]
        members = [lax.shift_right_logical(z_at[far], heads.bit_length() - 1) + half for far in fars for half in range(2)]
        cols = jnp.zeros((heads * props, 128), F32)
        for j, s in enumerate(members):
            raw = dot_last(q_scr[s], kbuf[s])
            minus = jnp.where(place < lengths[s], -logcum[s], NEG_LARGE)
            cum = cum_scr[pl.ds(pl.multiple_of(s * props, props), props), :]
            scores = jnp.concatenate(
                [
                    raw[h * props : (h + 1) * props] * scaling
                    + (cum[:, h : h + 1] + minus[h : h + 1])
                    for h in range(heads)
                ],
                axis=0,
            )
            top = jnp.maximum(jnp.max(scores, axis=-1, keepdims=True), NEG_FLOOR)
            weights = jnp.exp(scores - top)
            total = jnp.sum(weights, axis=-1, keepdims=True)
            some = total > 0.0
            safe = jnp.where(some, total, 1.0)
            out = jnp.dot(weights.astype(BF16), vbuf[s], preferred_element_type=F32)
            out = (out * (1.0 / safe)).astype(BF16)
            o_send[pl.ds(s * heads, heads)] = out.reshape(heads, props, head)
            lse = jnp.where(some, top + jnp.log(safe), NEG_LARGE)
            cols = jnp.where(slot == j, lse, cols)
        lse_rows = jnp.concatenate(
            [cols, jnp.zeros((128 - heads * props, 128), F32)], axis=0
        ).T
        for j, s in enumerate(members):
            lse_send[s] = lse_rows[j : j + 1]

        @pl.when(late)
        def _():
            if g == 0:
                pl.semaphore_wait(barrier, peers)
            send_planes(fars)

    @pl.when(jnp.logical_not(late))
    def _():
        pl.semaphore_wait(barrier, peers)
        send_planes(far_first)

    o_recv[me] = o_send[me]
    lse_recv[me] = lse_send[my_seq]

    for name in ("accepted", "pending_keys", "pending_values"):
        loads[name].wait()
    width = heads * props
    q_own = q_scr[my_seq]
    own_rows = pl.ds(pl.multiple_of(my_seq * props, props), props)
    extra = 16
    pad = jnp.zeros((extra - taken, head), F32)
    keys_x = jnp.concatenate(
        [
            kn_scr[own_rows, :].astype(F32),
            pending_keys[my_seq].astype(F32),
            pad,
        ],
        axis=0,
    ).astype(BF16)
    values_x = jnp.concatenate(
        [
            vn_scr[own_rows, :].astype(F32),
            pending_values[my_seq].astype(F32),
            pad,
        ],
        axis=0,
    ).astype(BF16)
    raw_t = dot_last(keys_x, q_own)
    cum_own = cum_scr[own_rows, :]
    lane_head = iota((props, width), 1) // props
    lane_prop = iota((props, width), 1) & (props - 1)
    cum_wide = jnp.zeros((props, width), F32)
    for h in range(heads):
        cum_wide = jnp.where(lane_head == h, cum_own[:, h : h + 1], cum_wide)
    cum_row = jnp.sum(
        jnp.where(lane_prop == iota((props, width), 0), cum_wide, 0.0), axis=0, keepdims=True
    )
    anc_fold = (
        (iota((rows, width), 0) & (props - 1)) == (iota((rows, width), 1) & (props - 1))
    ).astype(BF16)
    anc_own = jnp.dot(anc_scr[own_rows, :], anc_fold, preferred_element_type=F32)
    pend_wide = jnp.zeros((extra, width), F32)
    pend_sub = iota((extra, width), 0)
    for a in range(taken):
        col = jnp.sum(
            jnp.where(iota((heads, seqs), 1) == my_seq, pending_logcum[a], 0.0),
            axis=1,
            keepdims=True,
        )
        row = jnp.sum(
            jnp.where(iota((heads, width), 1) // props == iota((heads, width), 0), col, 0.0),
            axis=0,
            keepdims=True,
        )
        pend_wide = jnp.where(pend_sub == a, row, pend_wide)
    tree_t = jnp.where(
        anc_own > 0.5, raw_t[:props] * scaling + cum_row - cum_wide, NEG_LARGE
    )
    pend_t = jnp.where(
        pend_sub < accepted[my_seq], raw_t[props:] * scaling + cum_row - pend_wide, NEG_LARGE
    )
    both_t = jnp.concatenate([tree_t, pend_t], axis=0)
    top_t = jnp.max(both_t, axis=0, keepdims=True)
    weights_t = jnp.exp(both_t - top_t)
    total_t = jnp.sum(weights_t, axis=0, keepdims=True)
    share_t = (weights_t * (1.0 / total_t)).astype(BF16)
    tree_scr[...] = lax.dot_general(
        share_t, values_x, (((0,), (0,)), ((), ())), preferred_element_type=F32
    )
    head_rows = pl.ds(pl.multiple_of(my_head * props, props), props)
    o_recv[peers] = tree_scr[head_rows, :].astype(BF16)
    lse_t = top_t + jnp.log(total_t)
    lse_recv[peers] = jnp.concatenate([lse_t, jnp.zeros((1, 128 - width), F32)], axis=1)

    all_but_one(lse_recv, 1).wait_recv()
    slots = peers + 8
    lse_all = lse_recv[:, 0, :]
    weight = jnp.exp(lse_all - jnp.max(lse_all, axis=0, keepdims=True)).astype(BF16)
    pick = (
        (iota((128, 128), 0) - my_head * props) == (iota((128, 128), 1) & (props - 1))
    ).astype(BF16)
    picked = jnp.dot(weight, pick, preferred_element_type=F32)
    mine_8 = iota((8, 128), 1) // props == iota((8, 128), 0)
    mine_16 = (iota((props, 128), 1) & (props - 1)) == iota((props, 128), 0)
    mixes = []
    for c in range(slots // 8):
        flat = jnp.sum(
            jnp.where(mine_8, picked[c * 8 : (c + 1) * 8], 0.0), axis=0, keepdims=True
        )
        mixes.append(jnp.where(mine_16, flat, 0.0))
    den = functools.reduce(lambda a, b: a + b, mixes)
    den = jnp.sum(den, axis=1, keepdims=True)
    mix = jnp.concatenate(mixes, axis=1).astype(BF16)
    all_but_one(o_recv, 0).wait_recv()
    blended = jnp.dot(
        mix, o_recv[...].reshape(slots * props, head), preferred_element_type=F32
    )
    att[my_head * seqs + my_seq] = (blended / den).astype(BF16)

    for dz, dy in others:
        send_att(z_at[dz] + y_at[dy]).start()

    all_but_one(att, 2).wait_recv()

    loads["out_weight"].wait()
    part_t = jnp.zeros((out_weight.shape[0], rows), F32)
    for h in range(heads):
        part_t += dot_last(
            out_weight[:, h * head : (h + 1) * head],
            att[pl.ds(h * seqs, seqs)].reshape(rows, head),
        )
    half = out_weight.shape[0] // 2
    low, high = part_t[:half].astype(BF16), part_t[half:].astype(BF16)
    swap_send[...] = jnp.where(core == 0, high, low)
    swap = pltpu.make_async_remote_copy(
        src_ref=swap_send,
        dst_ref=swap_recv,
        send_sem=send_sem.at[3],
        recv_sem=recv_sem.at[3],
        device_id={"tp": 1 - core},
        device_id_type=MESH,
    )
    swap.start()
    kept = jnp.where(core == 0, low, high).astype(F32)
    swap.wait()
    final = kept + swap_recv[...].astype(F32)
    result[...] = final.T.astype(BF16).reshape(seqs, props, half)

    all_but_one(o_send, 0).wait_send()
    all_but_one(lse_recv, 1).wait_send()
    all_but_one(att, 2).wait_send()


def shards(
    tokens,
    norm_gain,
    query_weight,
    key_weight,
    value_weight,
    forget_weight,
    forget_bias,
    query_gain,
    key_gain,
    output_weight,
    cache_keys,
    cache_values,
    cache_logcum,
    pending_keys,
    pending_values,
    pending_logcum,
    lengths,
    accepted,
    parents,
):
    seqs, props, width = tokens.shape
    head = query_gain.shape[0]
    heads = query_weight.shape[1] // head
    block = cache_keys.shape[1]
    taken = pending_keys.shape[1]
    rows = seqs * props
    peers = seqs * heads
    half = output_weight.shape[1] // 2
    operands = {
        "tokens": tokens.reshape(rows, width),
        "norm_gain": norm_gain.reshape(1, width),
        "query_weight": query_weight,
        "key_weight": key_weight,
        "value_weight": value_weight,
        "forget": forget_weight.T,
        "forget_bias": forget_bias,
        "query_gain": query_gain.reshape(1, head),
        "key_gain": key_gain.reshape(1, head),
        "out_weight": output_weight.T,
        "keys": cache_keys.reshape(seqs, block, head),
        "values": cache_values.reshape(seqs, block, head),
        "logcum": jnp.swapaxes(cache_logcum, 1, 2),
        "pending_keys": pending_keys.reshape(seqs, taken, head),
        "pending_values": pending_values.reshape(seqs, taken, head),
        "pending_logcum": jnp.transpose(pending_logcum, (1, 2, 0)),
        "lengths": lengths,
        "accepted": accepted,
        "accepted_row": accepted.reshape(1, seqs),
        "parents": parents,
    }
    places = {
        name: (pltpu.SMEM if name in SCALARS else pltpu.VMEM)(array.shape, array.dtype)
        for name, array in operands.items()
        if name != "value_weight"
    }
    places["key_weight"] = pltpu.VMEM((width, 2 * head), BF16)
    return pl.pallas_call(
        functools.partial(kernel, seqs, heads, props, head, taken, block),
        out_shape=jax.ShapeDtypeStruct((seqs, props, half), BF16),
        in_specs=[{name: pl.BlockSpec(memory_space=pltpu.HBM) for name in operands}],
        out_specs=pl.BlockSpec(memory_space=pltpu.VMEM),
        scratch_shapes=[
            places,
            pltpu.VMEM((rows, width), BF16),
            pltpu.VMEM((rows, 128), F32),
            pltpu.VMEM((seqs, heads * props, head), BF16),
            pltpu.VMEM((rows, head), BF16),
            pltpu.VMEM((rows, head), BF16),
            pltpu.VMEM((rows, rows), BF16),
            pltpu.VMEM((rows, 2 * heads), F32),
            pltpu.VMEM((peers, props, head), BF16),
            pltpu.VMEM((peers + 8, props, head), BF16),
            pltpu.VMEM((seqs, 1, 128), F32),
            pltpu.VMEM((peers + 8, 1, 128), F32),
            pltpu.VMEM((heads * props, head), F32),
            pltpu.VMEM((peers, props, head), BF16),
            pltpu.VMEM((half, rows), BF16),
            pltpu.VMEM((half, rows), BF16),
            pltpu.SemaphoreType.DMA((len(operands),)),
            pltpu.SemaphoreType.DMA((4,)),
            pltpu.SemaphoreType.DMA((4,)),
        ],
        compiler_params=pltpu.CompilerParams(
            collective_id=0, has_side_effects=True, vmem_limit_bytes=48 * 1024 * 1024
        ),
    )(
        {
            name: pltpu.with_memory_space_constraint(array, pltpu.HBM)
            for name, array in operands.items()
        }
    )


def solution(mesh):
    placed = (
        P("dp", None, None),
        P(),
        P(None, "tp"),
        P(None, "tp"),
        P(None, "tp"),
        P(),
        P(),
        P(),
        P(),
        P("tp", "kv"),
        P("dp", "kv", "tp", None),
        P("dp", "kv", "tp", None),
        P("dp", "kv", "tp"),
        P("dp", None, "tp", None),
        P("dp", None, "tp", None),
        P("dp", None, "tp"),
        P("dp"),
        P("dp"),
        P("dp", None),
    )
    return jax.shard_map(
        shards, mesh=mesh, in_specs=placed, out_specs=P("dp", None, ("kv", "tp")), check_vma=False
    )
```

```python
import functools

import jax
import jax.numpy as jnp
from jax import lax
from jax.experimental import pallas as pl
from jax.experimental.pallas import tpu as pltpu
from jax.sharding import PartitionSpec as P

EPSILON = 1e-06
NEG_LARGE = -1e30
NEG_FLOOR = -1e29
ROUNDS = (2, 2, 2, 2)
HIGHEST = lax.Precision.HIGHEST
MESH = pl.DeviceIdType.MESH
F32 = jnp.float32
BF16 = jnp.bfloat16
LAST = (((1,), (1,)), ((), ()))
NAMES = (
    "tokens",
    "norm_gain",
    "query_weight",
    "key_weight",
    "value_weight",
    "forget",
    "forget_bias",
    "query_gain",
    "key_gain",
    "out_weight",
    "keys",
    "values",
    "logcum",
    "pending_keys",
    "pending_values",
    "pending_logcum",
    "lengths",
    "accepted",
    "accepted_row",
    "parents",
)
SCALARS = ("forget_bias", "lengths", "accepted")
LOAD_ORDER = (
    "parents",
    "tokens",
    "norm_gain",
    "forget",
    "forget_bias",
    "accepted_row",
    "pending_logcum",
    "key_gain",
    "query_gain",
    "key_weight",
    "value_weight",
    "query_weight",
    "keys",
    "logcum",
    "lengths",
    "values",
    "accepted",
    "pending_keys",
    "pending_values",
    "out_weight",
)


def iota(shape, dim):
    return lax.broadcasted_iota(jnp.int32, shape, dim)


def dot_last(a, b):
    return lax.dot_general(a, b, LAST, preferred_element_type=F32)


def by_distance(count):
    return sorted(range(count), key=lambda d: -min(d, count - d))


def unit(rows, gain):
    return rows * lax.rsqrt(jnp.mean(rows * rows, axis=-1, keepdims=True) + EPSILON) * gain


def kernel(
    seqs,
    heads,
    props,
    head,
    taken,
    block,
    operands,
    result,
    places,
    normed,
    scale_scr,
    q_scr,
    kn_scr,
    vn_scr,
    anc_scr,
    cum_scr,
    o_send,
    o_recv,
    lse_send,
    lse_recv,
    tree_scr,
    att,
    swap_send,
    swap_recv,
    load_sem,
    send_sem,
    recv_sem,
):
    rows = seqs * props
    peers = seqs * heads
    scaling = head**-0.5
    me = lax.axis_index("kv")
    core = lax.axis_index("tp")
    across_y = 2 * heads
    planes = seqs // 2
    my_z = me // across_y
    my_y = me & (across_y - 1)
    my_seq = me // heads
    my_head = me & (heads - 1)
    z_at = [((my_z + dz) & (planes - 1)) * across_y for dz in range(planes)]
    y_at = [(my_y + dy) & (across_y - 1) for dy in range(across_y)]
    others = sorted(
        ((dz, dy) for dz in range(planes) for dy in range(across_y) if dz or dy),
        key=lambda d: -min(d[0], planes - d[0]) - min(d[1], across_y - d[1]),
    )

    wkv = places["key_weight"]
    places = dict(
        places, key_weight=wkv.at[:, pl.ds(0, head)], value_weight=wkv.at[:, pl.ds(head, head)]
    )
    loads = {
        name: pltpu.make_async_copy(operands[name], places[name], load_sem.at[n])
        for n, name in enumerate(LOAD_ORDER)
    }
    for item in loads.values():
        item.start()
    (
        tok, norm_gain, wq, _, _, forget, forget_bias, query_gain, key_gain, out_weight,
        kbuf, vbuf, logcum, pending_keys, pending_values, pending_logcum, lengths, accepted,
        accepted_row, parents,
    ) = (places[name] for name in NAMES)

    barrier = pltpu.get_barrier_semaphore()

    for dz, dy in others:
        pl.semaphore_signal(
            barrier, inc=1, device_id={"kv": z_at[dz] + y_at[dy]}, device_id_type=MESH
        )
    pl.semaphore_signal(barrier, inc=1, device_id={"tp": 1 - core}, device_id_type=MESH)

    loads["parents"].wait()

    lane = iota((seqs, rows), 1)
    spread = ((iota((props, rows), 1) & (props - 1)) == iota((props, rows), 0)).astype(BF16)
    repeated = jnp.dot(
        parents[...].astype(F32).astype(BF16), spread, preferred_element_type=F32
    )
    parent_row = jnp.sum(
        jnp.where(lane // props == iota((seqs, rows), 0), repeated, 0.0), axis=0, keepdims=True
    ).astype(jnp.int32)
    down = iota((rows, rows), 0)
    across = iota((rows, rows), 1)
    same = down // props == across // props
    linked = (same & (parent_row == (down & (props - 1)))) | (down == across)
    anc_t = jnp.where(linked, 1.0, 0.0).astype(BF16)
    for _ in range((props - 1).bit_length()):
        anc_t = jnp.minimum(jnp.dot(anc_t, anc_t, preferred_element_type=F32), 1.0).astype(BF16)
    anc_scr[...] = anc_t

    loads["tokens"].wait()
    loads["norm_gain"].wait()

    model = tok.shape[1]

    @pl.loop(0, rows // 32)
    def _(step):
        piece = pl.ds(step * 32, 32)
        total = jnp.zeros((32, 128), F32)
        for c in range(model // 128):
            wide = tok[piece, c * 128 : (c + 1) * 128].astype(F32)
            total += wide * wide
        scale_scr[piece, :] = total

    mean = jnp.sum(scale_scr[...], axis=1, keepdims=True) * (1.0 / model)
    scale_scr[...] = jnp.broadcast_to(lax.rsqrt(mean + EPSILON), (rows, 128))

    @pl.loop(0, rows // 32)
    def _(step):
        piece = pl.ds(step * 32, 32)
        scale = scale_scr[piece, :]
        for c in range(model // 128):
            columns = slice(c * 128, (c + 1) * 128)
            wide = tok[piece, columns].astype(F32)
            normed[piece, columns] = (wide * scale * norm_gain[:, columns]).astype(BF16)

    for name in (
        "forget", "forget_bias", "accepted_row", "pending_logcum", "key_gain", "query_gain",
        "key_weight", "value_weight", "query_weight",
    ):
        loads[name].wait()
    gate_raw = dot_last(forget[...], normed[...])
    gate_head = iota((2 * heads, 1), 0)
    bias = jnp.zeros((2 * heads, 1), F32)
    for n in range(2 * heads):
        bias = jnp.where(gate_head == n, forget_bias[n], bias)
    gate_raw = gate_raw + bias
    gates = jnp.minimum(gate_raw, 0.0) - jnp.log1p(jnp.exp(-jnp.abs(gate_raw)))
    gates = jnp.where(
        core == 0, gates, jnp.concatenate([gates[heads:], gates[:heads]], axis=0)
    )
    base = jnp.zeros((heads, seqs), F32)
    for a in range(taken):
        base = jnp.where(accepted_row[...] - 1 == a, pending_logcum[a], base)
    base = jnp.concatenate([base, jnp.zeros((heads, seqs), F32)], axis=0)
    expand = (lane // props == iota((seqs, rows), 0)).astype(F32)
    cum_t = jnp.dot(
        gates, anc_t.astype(F32), precision=HIGHEST, preferred_element_type=F32
    ) + jnp.dot(base, expand, precision=HIGHEST, preferred_element_type=F32)
    cum_scr[...] = cum_t.T

    sides = jnp.dot(normed[...], wkv[...], preferred_element_type=F32)
    kn_scr[...] = unit(sides[:, :head], key_gain[...]).astype(BF16)
    vn_scr[...] = sides[:, head:].astype(BF16)
    for pair in range(heads // 2):
        raw = jnp.dot(
            normed[...],
            wq[:, 2 * pair * head : (2 * pair + 2) * head],
            preferred_element_type=F32,
        )
        for h in (2 * pair, 2 * pair + 1):
            one = raw[:, (h - 2 * pair) * head : (h - 2 * pair + 1) * head]
            q_scr[:, h * props : (h + 1) * props, :] = (
                unit(one, query_gain[...]).astype(BF16).reshape(seqs, props, head)
            )

    o_recv[pl.ds(peers, 8)] = jnp.zeros((8, props, head), BF16)
    lse_recv[pl.ds(peers, 8)] = jnp.full((8, 1, 128), NEG_LARGE, F32)

    for name in ("keys", "logcum", "lengths", "values"):
        loads[name].wait()
    def send_out(k):
        return pltpu.make_async_remote_copy(
            src_ref=o_send.at[k],
            dst_ref=o_recv.at[me],
            send_sem=send_sem.at[0],
            recv_sem=recv_sem.at[0],
            device_id={"kv": k},
            device_id_type=MESH,
        )

    def send_lse(k):
        return pltpu.make_async_remote_copy(
            src_ref=lse_send.at[lax.shift_right_logical(k, heads.bit_length() - 1)],
            dst_ref=lse_recv.at[me],
            send_sem=send_sem.at[1],
            recv_sem=recv_sem.at[1],
            device_id={"kv": k},
            device_id_type=MESH,
        )

    def send_att(k):
        mine = att.at[my_head * seqs + my_seq]
        return pltpu.make_async_remote_copy(
            src_ref=mine,
            dst_ref=mine,
            send_sem=send_sem.at[2],
            recv_sem=recv_sem.at[2],
            device_id={"kv": k},
            device_id_type=MESH,
        )

    def all_but_one(ref, n):
        some = ref.at[pl.ds(0, peers - 1)]
        return pltpu.make_async_remote_copy(
            src_ref=some,
            dst_ref=some,
            send_sem=send_sem.at[n],
            recv_sem=recv_sem.at[n],
            device_id={"kv": me},
            device_id_type=MESH,
        )

    def send_planes(fars):
        for far in fars:
            for dy in by_distance(across_y):
                if far or dy:
                    send_out(z_at[far] + y_at[dy]).start()
                    send_lse(z_at[far] + y_at[dy]).start()

    place = me * block + iota((1, block), 1)
    slot = iota((heads * props, 128), 1)
    late = my_z >= planes // 2
    far_first = by_distance(planes)
    far_rounds = [
        far_first[sum(ROUNDS[:g]) * planes // 8 : sum(ROUNDS[: g + 1]) * planes // 8]
        for g in range(len(ROUNDS))
    ]
    members = [
        [
            lax.shift_right_logical(z_at[far], heads.bit_length() - 1) + half
            for far in fars
            for half in range(2)
        ]
        for fars in far_rounds
    ]
    ahead = [dot_last(q_scr[s], kbuf[s]) for s in members[0]]
    for g, fars in enumerate(far_rounds):
        raws = ahead
        ahead = [dot_last(q_scr[s], kbuf[s]) for s in members[g + 1]] if g + 1 < len(members) else []
        cols = jnp.zeros((heads * props, 128), F32)
        for j, (s, raw) in enumerate(zip(members[g], raws)):
            minus = jnp.where(place < lengths[s], -logcum[s], NEG_LARGE)
            cum = cum_scr[pl.ds(pl.multiple_of(s * props, props), props), :]
            scores = jnp.concatenate(
                [
                    raw[h * props : (h + 1) * props] * scaling
                    + (cum[:, h : h + 1] + minus[h : h + 1])
                    for h in range(heads)
                ],
                axis=0,
            )
            top = jnp.maximum(jnp.max(scores, axis=-1, keepdims=True), NEG_FLOOR)
            weights = jnp.exp(scores - top)
            total = jnp.sum(weights, axis=-1, keepdims=True)
            out = jnp.dot(weights.astype(BF16), vbuf[s], preferred_element_type=F32)
            out = (out * (1.0 / jnp.maximum(total, 1.0))).astype(BF16)
            o_send[pl.ds(s * heads, heads)] = out.reshape(heads, props, head)
            cols = jnp.where(slot == j, top, jnp.where(slot == 16 + j, total, cols))
        turned = jnp.concatenate(
            [cols, jnp.zeros((128 - heads * props, 128), F32)], axis=0
        ).T
        totals = turned[16:32]
        lse_rows = jnp.where(
            totals > 0.0, turned[:16] + jnp.log(jnp.maximum(totals, 1.0)), NEG_LARGE
        )
        for j, s in enumerate(members[g]):
            lse_send[s] = lse_rows[j : j + 1]

        @pl.when(late)
        def _():
            if g == 0:
                pl.semaphore_wait(barrier, peers)
            send_planes(fars)

    @pl.when(jnp.logical_not(late))
    def _():
        pl.semaphore_wait(barrier, peers)
        send_planes(far_first)

    o_recv[me] = o_send[me]
    lse_recv[me] = lse_send[my_seq]

    for name in ("accepted", "pending_keys", "pending_values"):
        loads[name].wait()
    width = heads * props
    q_own = q_scr[my_seq]
    own_rows = pl.ds(pl.multiple_of(my_seq * props, props), props)
    extra = 16
    pad = jnp.zeros((extra - taken, head), F32)
    keys_x = jnp.concatenate(
        [
            kn_scr[own_rows, :].astype(F32),
            pending_keys[my_seq].astype(F32),
            pad,
        ],
        axis=0,
    ).astype(BF16)
    values_x = jnp.concatenate(
        [
            vn_scr[own_rows, :].astype(F32),
            pending_values[my_seq].astype(F32),
            pad,
        ],
        axis=0,
    ).astype(BF16)
    raw_t = dot_last(keys_x, q_own)
    cum_own = cum_scr[own_rows, :]
    lane_head = iota((props, width), 1) // props
    lane_prop = iota((props, width), 1) & (props - 1)
    cum_wide = jnp.zeros((props, width), F32)
    for h in range(heads):
        cum_wide = jnp.where(lane_head == h, cum_own[:, h : h + 1], cum_wide)
    cum_row = jnp.sum(
        jnp.where(lane_prop == iota((props, width), 0), cum_wide, 0.0), axis=0, keepdims=True
    )
    anc_fold = (
        (iota((rows, width), 0) & (props - 1)) == (iota((rows, width), 1) & (props - 1))
    ).astype(BF16)
    anc_own = jnp.dot(anc_scr[own_rows, :], anc_fold, preferred_element_type=F32)
    pend_wide = jnp.zeros((extra, width), F32)
    pend_sub = iota((extra, width), 0)
    for a in range(taken):
        col = jnp.sum(
            jnp.where(iota((heads, seqs), 1) == my_seq, pending_logcum[a], 0.0),
            axis=1,
            keepdims=True,
        )
        row = jnp.sum(
            jnp.where(iota((heads, width), 1) // props == iota((heads, width), 0), col, 0.0),
            axis=0,
            keepdims=True,
        )
        pend_wide = jnp.where(pend_sub == a, row, pend_wide)
    tree_t = jnp.where(
        anc_own > 0.5, raw_t[:props] * scaling + cum_row - cum_wide, NEG_LARGE
    )
    pend_t = jnp.where(
        pend_sub < accepted[my_seq], raw_t[props:] * scaling + cum_row - pend_wide, NEG_LARGE
    )
    both_t = jnp.concatenate([tree_t, pend_t], axis=0)
    top_t = jnp.max(both_t, axis=0, keepdims=True)
    weights_t = jnp.exp(both_t - top_t)
    total_t = jnp.sum(weights_t, axis=0, keepdims=True)
    share_t = (weights_t * (1.0 / total_t)).astype(BF16)
    tree_scr[...] = lax.dot_general(
        share_t, values_x, (((0,), (0,)), ((), ())), preferred_element_type=F32
    )
    head_rows = pl.ds(pl.multiple_of(my_head * props, props), props)
    o_recv[peers] = tree_scr[head_rows, :].astype(BF16)
    lse_t = top_t + jnp.log(total_t)
    lse_recv[peers] = jnp.concatenate([lse_t, jnp.zeros((1, 128 - width), F32)], axis=1)

    all_but_one(lse_recv, 1).wait_recv()
    slots = peers + 8
    lse_all = lse_recv[:, 0, :]
    weight = jnp.exp(lse_all - jnp.max(lse_all, axis=0, keepdims=True)).astype(BF16)
    pick = (
        (iota((128, 128), 0) - my_head * props) == (iota((128, 128), 1) & (props - 1))
    ).astype(BF16)
    picked = jnp.dot(weight, pick, preferred_element_type=F32)
    mine_8 = iota((8, 128), 1) // props == iota((8, 128), 0)
    mine_16 = (iota((props, 128), 1) & (props - 1)) == iota((props, 128), 0)
    mixes = []
    for c in range(slots // 8):
        flat = jnp.sum(
            jnp.where(mine_8, picked[c * 8 : (c + 1) * 8], 0.0), axis=0, keepdims=True
        )
        mixes.append(jnp.where(mine_16, flat, 0.0))
    den = functools.reduce(lambda a, b: a + b, mixes)
    den = jnp.sum(den, axis=1, keepdims=True)
    mix = jnp.concatenate(mixes, axis=1).astype(BF16)
    all_but_one(o_recv, 0).wait_recv()
    blended = jnp.dot(
        mix, o_recv[...].reshape(slots * props, head), preferred_element_type=F32
    )
    att[my_head * seqs + my_seq] = (blended / den).astype(BF16)

    for dz, dy in others:
        send_att(z_at[dz] + y_at[dy]).start()

    all_but_one(att, 2).wait_recv()

    loads["out_weight"].wait()
    part_t = jnp.zeros((out_weight.shape[0], rows), F32)
    for h in range(heads):
        part_t += dot_last(
            out_weight[:, h * head : (h + 1) * head],
            att[pl.ds(h * seqs, seqs)].reshape(rows, head),
        )
    half = out_weight.shape[0] // 2
    low, high = part_t[:half].astype(BF16), part_t[half:].astype(BF16)
    swap_send[...] = jnp.where(core == 0, high, low)
    swap = pltpu.make_async_remote_copy(
        src_ref=swap_send,
        dst_ref=swap_recv,
        send_sem=send_sem.at[3],
        recv_sem=recv_sem.at[3],
        device_id={"tp": 1 - core},
        device_id_type=MESH,
    )
    swap.start()
    kept = jnp.where(core == 0, low, high).astype(F32)
    swap.wait()
    final = kept + swap_recv[...].astype(F32)
    result[...] = final.T.astype(BF16).reshape(seqs, props, half)

    all_but_one(o_send, 0).wait_send()
    all_but_one(lse_recv, 1).wait_send()
    all_but_one(att, 2).wait_send()


def shards(
    tokens,
    norm_gain,
    query_weight,
    key_weight,
    value_weight,
    forget_weight,
    forget_bias,
    query_gain,
    key_gain,
    output_weight,
    cache_keys,
    cache_values,
    cache_logcum,
    pending_keys,
    pending_values,
    pending_logcum,
    lengths,
    accepted,
    parents,
):
    seqs, props, width = tokens.shape
    head = query_gain.shape[0]
    heads = query_weight.shape[1] // head
    block = cache_keys.shape[1]
    taken = pending_keys.shape[1]
    rows = seqs * props
    peers = seqs * heads
    half = output_weight.shape[1] // 2
    operands = {
        "tokens": tokens.reshape(rows, width),
        "norm_gain": norm_gain.reshape(1, width),
        "query_weight": query_weight,
        "key_weight": key_weight,
        "value_weight": value_weight,
        "forget": forget_weight.T,
        "forget_bias": forget_bias,
        "query_gain": query_gain.reshape(1, head),
        "key_gain": key_gain.reshape(1, head),
        "out_weight": output_weight.T,
        "keys": cache_keys.reshape(seqs, block, head),
        "values": cache_values.reshape(seqs, block, head),
        "logcum": jnp.swapaxes(cache_logcum, 1, 2),
        "pending_keys": pending_keys.reshape(seqs, taken, head),
        "pending_values": pending_values.reshape(seqs, taken, head),
        "pending_logcum": jnp.transpose(pending_logcum, (1, 2, 0)),
        "lengths": lengths,
        "accepted": accepted,
        "accepted_row": accepted.reshape(1, seqs),
        "parents": parents,
    }
    places = {
        name: (pltpu.SMEM if name in SCALARS else pltpu.VMEM)(array.shape, array.dtype)
        for name, array in operands.items()
        if name != "value_weight"
    }
    places["key_weight"] = pltpu.VMEM((width, 2 * head), BF16)
    return pl.pallas_call(
        functools.partial(kernel, seqs, heads, props, head, taken, block),
        out_shape=jax.ShapeDtypeStruct((seqs, props, half), BF16),
        in_specs=[{name: pl.BlockSpec(memory_space=pltpu.HBM) for name in operands}],
        out_specs=pl.BlockSpec(memory_space=pltpu.VMEM),
        scratch_shapes=[
            places,
            pltpu.VMEM((rows, width), BF16),
            pltpu.VMEM((rows, 128), F32),
            pltpu.VMEM((seqs, heads * props, head), BF16),
            pltpu.VMEM((rows, head), BF16),
            pltpu.VMEM((rows, head), BF16),
            pltpu.VMEM((rows, rows), BF16),
            pltpu.VMEM((rows, 2 * heads), F32),
            pltpu.VMEM((peers, props, head), BF16),
            pltpu.VMEM((peers + 8, props, head), BF16),
            pltpu.VMEM((seqs, 1, 128), F32),
            pltpu.VMEM((peers + 8, 1, 128), F32),
            pltpu.VMEM((heads * props, head), F32),
            pltpu.VMEM((peers, props, head), BF16),
            pltpu.VMEM((half, rows), BF16),
            pltpu.VMEM((half, rows), BF16),
            pltpu.SemaphoreType.DMA((len(operands),)),
            pltpu.SemaphoreType.DMA((4,)),
            pltpu.SemaphoreType.DMA((4,)),
        ],
        compiler_params=pltpu.CompilerParams(
            collective_id=0, has_side_effects=True, vmem_limit_bytes=48 * 1024 * 1024
        ),
    )(
        {
            name: pltpu.with_memory_space_constraint(array, pltpu.HBM)
            for name, array in operands.items()
        }
    )


def solution(mesh):
    placed = (
        P("dp", None, None),
        P(),
        P(None, "tp"),
        P(None, "tp"),
        P(None, "tp"),
        P(),
        P(),
        P(),
        P(),
        P("tp", "kv"),
        P("dp", "kv", "tp", None),
        P("dp", "kv", "tp", None),
        P("dp", "kv", "tp"),
        P("dp", None, "tp", None),
        P("dp", None, "tp", None),
        P("dp", None, "tp"),
        P("dp"),
        P("dp"),
        P("dp", None),
    )
    return jax.shard_map(
        shards, mesh=mesh, in_specs=placed, out_specs=P("dp", None, ("kv", "tp")), check_vma=False
    )
```

```python
import functools

import jax
import jax.numpy as jnp
from jax import lax
from jax.experimental import pallas as pl
from jax.experimental.pallas import tpu as pltpu
from jax.sharding import PartitionSpec as P

EPSILON = 1e-06
NEG_LARGE = -1e30
NEG_FLOOR = -1e29
ROUNDS = (2, 2, 2, 2)
HIGHEST = lax.Precision.HIGHEST
MESH = pl.DeviceIdType.MESH
F32 = jnp.float32
BF16 = jnp.bfloat16
LAST = (((1,), (1,)), ((), ()))
NAMES = (
    "tokens",
    "norm_gain",
    "query_weight",
    "key_weight",
    "value_weight",
    "forget",
    "forget_bias",
    "query_gain",
    "key_gain",
    "out_weight",
    "keys",
    "values",
    "logcum",
    "pending_keys",
    "pending_values",
    "pending_logcum",
    "lengths",
    "accepted",
    "accepted_row",
    "parents",
)
SCALARS = ("forget_bias", "lengths", "accepted")
LOAD_ORDER = (
    "parents",
    "tokens",
    "norm_gain",
    "forget",
    "forget_bias",
    "accepted_row",
    "pending_logcum",
    "key_gain",
    "query_gain",
    "key_weight",
    "value_weight",
    "query_weight",
    "keys",
    "logcum",
    "lengths",
    "values",
    "accepted",
    "pending_keys",
    "pending_values",
    "out_weight",
)


def iota(shape, dim):
    return lax.broadcasted_iota(jnp.int32, shape, dim)


def dot_last(a, b):
    return lax.dot_general(a, b, LAST, preferred_element_type=F32)


def by_distance(count):
    return sorted(range(count), key=lambda d: -min(d, count - d))


def unit(rows, gain):
    return rows * lax.rsqrt(jnp.mean(rows * rows, axis=-1, keepdims=True) + EPSILON) * gain


def kernel(
    seqs,
    heads,
    props,
    head,
    taken,
    block,
    operands,
    result,
    places,
    normed,
    scale_scr,
    q_scr,
    kn_scr,
    vn_scr,
    anc_scr,
    cum_scr,
    o_send,
    o_recv,
    lse_send,
    lse_recv,
    tree_scr,
    att,
    swap_send,
    swap_recv,
    load_sem,
    send_sem,
    recv_sem,
):
    rows = seqs * props
    peers = seqs * heads
    scaling = head**-0.5
    me = lax.axis_index("kv")
    core = lax.axis_index("tp")
    across_y = 2 * heads
    planes = seqs // 2
    my_z = me // across_y
    my_y = me & (across_y - 1)
    my_seq = me // heads
    my_head = me & (heads - 1)
    z_at = [((my_z + dz) & (planes - 1)) * across_y for dz in range(planes)]
    y_at = [(my_y + dy) & (across_y - 1) for dy in range(across_y)]
    others = sorted(
        ((dz, dy) for dz in range(planes) for dy in range(across_y) if dz or dy),
        key=lambda d: -min(d[0], planes - d[0]) - min(d[1], across_y - d[1]),
    )

    wkv = places["key_weight"]
    places = dict(
        places, key_weight=wkv.at[:, pl.ds(0, head)], value_weight=wkv.at[:, pl.ds(head, head)]
    )
    loads = {
        name: pltpu.make_async_copy(operands[name], places[name], load_sem.at[n])
        for n, name in enumerate(LOAD_ORDER)
    }
    for item in loads.values():
        item.start()
    (
        tok, norm_gain, wq, _, _, forget, forget_bias, query_gain, key_gain, out_weight,
        kbuf, vbuf, logcum, pending_keys, pending_values, pending_logcum, lengths, accepted,
        accepted_row, parents,
    ) = (places[name] for name in NAMES)

    barrier = pltpu.get_barrier_semaphore()

    for dz, dy in others:
        pl.semaphore_signal(
            barrier, inc=1, device_id={"kv": z_at[dz] + y_at[dy]}, device_id_type=MESH
        )
    pl.semaphore_signal(barrier, inc=1, device_id={"tp": 1 - core}, device_id_type=MESH)

    loads["parents"].wait()

    lane = iota((seqs, rows), 1)
    spread = ((iota((props, rows), 1) & (props - 1)) == iota((props, rows), 0)).astype(BF16)
    repeated = jnp.dot(
        parents[...].astype(F32).astype(BF16), spread, preferred_element_type=F32
    )
    parent_row = jnp.sum(
        jnp.where(lane // props == iota((seqs, rows), 0), repeated, 0.0), axis=0, keepdims=True
    ).astype(jnp.int32)
    side = anc_scr.shape[1]
    down = iota((side, side), 0)
    across = iota((side, side), 1)
    same = down // props == across // props
    anc_t = []
    for start in range(0, rows, side):
        linked = (same & (parent_row[:, start : start + side] == (down & (props - 1)))) | (
            down == across
        )
        reach = jnp.where(linked, 1.0, 0.0).astype(BF16)
        for _ in range((props - 1).bit_length()):
            reach = jnp.minimum(
                jnp.dot(reach, reach, preferred_element_type=F32), 1.0
            ).astype(BF16)
        anc_scr[start : start + side, :] = reach
        anc_t.append(reach)

    loads["tokens"].wait()
    loads["norm_gain"].wait()

    model = tok.shape[1]

    @pl.loop(0, rows // 32)
    def _(step):
        piece = pl.ds(step * 32, 32)
        total = jnp.zeros((32, 128), F32)
        for c in range(model // 128):
            wide = tok[piece, c * 128 : (c + 1) * 128].astype(F32)
            total += wide * wide
        scale_scr[piece, :] = total

    mean = jnp.sum(scale_scr[...], axis=1, keepdims=True) * (1.0 / model)
    scale_scr[...] = jnp.broadcast_to(lax.rsqrt(mean + EPSILON), (rows, 128))

    @pl.loop(0, rows // 32)
    def _(step):
        piece = pl.ds(step * 32, 32)
        scale = scale_scr[piece, :]
        for c in range(model // 128):
            columns = slice(c * 128, (c + 1) * 128)
            wide = tok[piece, columns].astype(F32)
            normed[piece, columns] = (wide * scale * norm_gain[:, columns]).astype(BF16)

    for name in (
        "forget", "forget_bias", "accepted_row", "pending_logcum", "key_gain", "query_gain",
        "key_weight", "value_weight", "query_weight",
    ):
        loads[name].wait()
    gate_raw = dot_last(forget[...], normed[...])
    gate_head = iota((2 * heads, 1), 0)
    bias = jnp.zeros((2 * heads, 1), F32)
    for n in range(2 * heads):
        bias = jnp.where(gate_head == n, forget_bias[n], bias)
    gate_raw = gate_raw + bias
    gates = jnp.minimum(gate_raw, 0.0) - jnp.log1p(jnp.exp(-jnp.abs(gate_raw)))
    gates = jnp.where(
        core == 0, gates, jnp.concatenate([gates[heads:], gates[:heads]], axis=0)
    )
    base = jnp.zeros((heads, seqs), F32)
    for a in range(taken):
        base = jnp.where(accepted_row[...] - 1 == a, pending_logcum[a], base)
    base = jnp.concatenate([base, jnp.zeros((heads, seqs), F32)], axis=0)
    expand = (lane // props == iota((seqs, rows), 0)).astype(F32)
    cum_t = jnp.concatenate(
        [
            jnp.dot(
                gates[:, n * side : (n + 1) * side],
                reach.astype(F32),
                precision=HIGHEST,
                preferred_element_type=F32,
            )
            for n, reach in enumerate(anc_t)
        ],
        axis=1,
    ) + jnp.dot(base, expand, precision=HIGHEST, preferred_element_type=F32)
    cum_scr[...] = cum_t.T

    sides = jnp.dot(normed[...], wkv[...], preferred_element_type=F32)
    kn_scr[...] = unit(sides[:, :head], key_gain[...]).astype(BF16)
    vn_scr[...] = sides[:, head:].astype(BF16)
    for pair in range(heads // 2):
        raw = jnp.dot(
            normed[...],
            wq[:, 2 * pair * head : (2 * pair + 2) * head],
            preferred_element_type=F32,
        )
        for h in (2 * pair, 2 * pair + 1):
            one = raw[:, (h - 2 * pair) * head : (h - 2 * pair + 1) * head]
            q_scr[:, h * props : (h + 1) * props, :] = (
                unit(one, query_gain[...]).astype(BF16).reshape(seqs, props, head)
            )

    o_recv[pl.ds(peers, 8)] = jnp.zeros((8, props, head), BF16)
    lse_recv[pl.ds(peers, 8)] = jnp.full((8, 1, 128), NEG_LARGE, F32)

    for name in ("keys", "logcum", "lengths", "values"):
        loads[name].wait()
    def send_out(k):
        return pltpu.make_async_remote_copy(
            src_ref=o_send.at[k],
            dst_ref=o_recv.at[me],
            send_sem=send_sem.at[0],
            recv_sem=recv_sem.at[0],
            device_id={"kv": k},
            device_id_type=MESH,
        )

    def send_lse(k):
        return pltpu.make_async_remote_copy(
            src_ref=lse_send.at[lax.shift_right_logical(k, heads.bit_length() - 1)],
            dst_ref=lse_recv.at[me],
            send_sem=send_sem.at[1],
            recv_sem=recv_sem.at[1],
            device_id={"kv": k},
            device_id_type=MESH,
        )

    def send_att(k):
        mine = att.at[my_head * seqs + my_seq]
        return pltpu.make_async_remote_copy(
            src_ref=mine,
            dst_ref=mine,
            send_sem=send_sem.at[2],
            recv_sem=recv_sem.at[2],
            device_id={"kv": k},
            device_id_type=MESH,
        )

    def all_but_one(ref, n):
        some = ref.at[pl.ds(0, peers - 1)]
        return pltpu.make_async_remote_copy(
            src_ref=some,
            dst_ref=some,
            send_sem=send_sem.at[n],
            recv_sem=recv_sem.at[n],
            device_id={"kv": me},
            device_id_type=MESH,
        )

    def send_planes(fars):
        for far in fars:
            for dy in by_distance(across_y):
                if far or dy:
                    send_lse(z_at[far] + y_at[dy]).start()
                    send_out(z_at[far] + y_at[dy]).start()

    place = me * block + iota((1, block), 1)
    slot = iota((heads * props, 128), 1)
    late = my_z >= planes // 2
    far_first = by_distance(planes)
    far_rounds = [
        far_first[sum(ROUNDS[:g]) * planes // 8 : sum(ROUNDS[: g + 1]) * planes // 8]
        for g in range(len(ROUNDS))
    ]
    members = [
        [
            lax.shift_right_logical(z_at[far], heads.bit_length() - 1) + half
            for far in fars
            for half in range(2)
        ]
        for fars in far_rounds
    ]
    ahead = [dot_last(q_scr[s], kbuf[s]) for s in members[0]]
    for g, fars in enumerate(far_rounds):
        raws = ahead
        ahead = [dot_last(q_scr[s], kbuf[s]) for s in members[g + 1]] if g + 1 < len(members) else []
        cols = jnp.zeros((heads * props, 128), F32)
        for j, (s, raw) in enumerate(zip(members[g], raws)):
            minus = jnp.where(place < lengths[s], -logcum[s], NEG_LARGE)
            cum = cum_scr[pl.ds(pl.multiple_of(s * props, props), props), :]
            scores = jnp.concatenate(
                [
                    raw[h * props : (h + 1) * props] * scaling
                    + (cum[:, h : h + 1] + minus[h : h + 1])
                    for h in range(heads)
                ],
                axis=0,
            )
            top = jnp.maximum(jnp.max(scores, axis=-1, keepdims=True), NEG_FLOOR)
            weights = jnp.exp(scores - top)
            total = jnp.sum(weights, axis=-1, keepdims=True)
            out = jnp.dot(weights.astype(BF16), vbuf[s], preferred_element_type=F32)
            out = (out * (1.0 / jnp.maximum(total, 1.0))).astype(BF16)
            o_send[pl.ds(s * heads, heads)] = out.reshape(heads, props, head)
            cols = jnp.where(slot == j, top, jnp.where(slot == 16 + j, total, cols))
        turned = jnp.concatenate(
            [cols, jnp.zeros((128 - heads * props, 128), F32)], axis=0
        ).T
        totals = turned[16:32]
        lse_rows = jnp.where(
            totals > 0.0, turned[:16] + jnp.log(jnp.maximum(totals, 1.0)), NEG_LARGE
        )
        for j, s in enumerate(members[g]):
            lse_send[s] = lse_rows[j : j + 1]

        @pl.when(late)
        def _():
            if g == 0:
                pl.semaphore_wait(barrier, peers)
            send_planes(fars)

    @pl.when(jnp.logical_not(late))
    def _():
        pl.semaphore_wait(barrier, peers)
        send_planes(far_first)

    o_recv[me] = o_send[me]
    lse_recv[me] = lse_send[my_seq]

    for name in ("accepted", "pending_keys", "pending_values"):
        loads[name].wait()
    width = heads * props
    q_own = q_scr[my_seq]
    own_rows = pl.ds(pl.multiple_of(my_seq * props, props), props)
    extra = 16
    pad = jnp.zeros((extra - taken, head), F32)
    keys_x = jnp.concatenate(
        [
            kn_scr[own_rows, :].astype(F32),
            pending_keys[my_seq].astype(F32),
            pad,
        ],
        axis=0,
    ).astype(BF16)
    values_x = jnp.concatenate(
        [
            vn_scr[own_rows, :].astype(F32),
            pending_values[my_seq].astype(F32),
            pad,
        ],
        axis=0,
    ).astype(BF16)
    raw_t = dot_last(keys_x, q_own)
    cum_own = cum_scr[own_rows, :]
    lane_head = iota((props, width), 1) // props
    lane_prop = iota((props, width), 1) & (props - 1)
    cum_wide = jnp.zeros((props, width), F32)
    for h in range(heads):
        cum_wide = jnp.where(lane_head == h, cum_own[:, h : h + 1], cum_wide)
    cum_row = jnp.sum(
        jnp.where(lane_prop == iota((props, width), 0), cum_wide, 0.0), axis=0, keepdims=True
    )
    anc_fold = (
        (iota((side, width), 0) & (props - 1)) == (iota((side, width), 1) & (props - 1))
    ).astype(BF16)
    anc_own = jnp.dot(anc_scr[own_rows, :], anc_fold, preferred_element_type=F32)
    pend_wide = jnp.zeros((extra, width), F32)
    pend_sub = iota((extra, width), 0)
    for a in range(taken):
        col = jnp.sum(
            jnp.where(iota((heads, seqs), 1) == my_seq, pending_logcum[a], 0.0),
            axis=1,
            keepdims=True,
        )
        row = jnp.sum(
            jnp.where(iota((heads, width), 1) // props == iota((heads, width), 0), col, 0.0),
            axis=0,
            keepdims=True,
        )
        pend_wide = jnp.where(pend_sub == a, row, pend_wide)
    tree_t = jnp.where(
        anc_own > 0.5, raw_t[:props] * scaling + cum_row - cum_wide, NEG_LARGE
    )
    pend_t = jnp.where(
        pend_sub < accepted[my_seq], raw_t[props:] * scaling + cum_row - pend_wide, NEG_LARGE
    )
    both_t = jnp.concatenate([tree_t, pend_t], axis=0)
    top_t = jnp.max(both_t, axis=0, keepdims=True)
    weights_t = jnp.exp(both_t - top_t)
    total_t = jnp.sum(weights_t, axis=0, keepdims=True)
    share_t = (weights_t * (1.0 / total_t)).astype(BF16)
    tree_scr[...] = lax.dot_general(
        share_t, values_x, (((0,), (0,)), ((), ())), preferred_element_type=F32
    )
    head_rows = pl.ds(pl.multiple_of(my_head * props, props), props)
    o_recv[peers] = tree_scr[head_rows, :].astype(BF16)
    lse_t = top_t + jnp.log(total_t)
    lse_recv[peers] = jnp.concatenate([lse_t, jnp.zeros((1, 128 - width), F32)], axis=1)

    all_but_one(lse_recv, 1).wait_recv()
    slots = peers + 8
    lse_all = lse_recv[:, 0, :]
    weight = jnp.exp(lse_all - jnp.max(lse_all, axis=0, keepdims=True)).astype(BF16)
    pick = (
        (iota((128, 128), 0) - my_head * props) == (iota((128, 128), 1) & (props - 1))
    ).astype(BF16)
    picked = jnp.dot(weight, pick, preferred_element_type=F32)
    mine_8 = iota((8, 128), 1) // props == iota((8, 128), 0)
    mine_16 = (iota((props, 128), 1) & (props - 1)) == iota((props, 128), 0)
    mixes = []
    for c in range(slots // 8):
        flat = jnp.sum(
            jnp.where(mine_8, picked[c * 8 : (c + 1) * 8], 0.0), axis=0, keepdims=True
        )
        mixes.append(jnp.where(mine_16, flat, 0.0))
    den = functools.reduce(lambda a, b: a + b, mixes)
    den = jnp.sum(den, axis=1, keepdims=True)
    mix = jnp.concatenate(mixes, axis=1).astype(BF16)
    all_but_one(o_recv, 0).wait_recv()
    blended = jnp.dot(
        mix, o_recv[...].reshape(slots * props, head), preferred_element_type=F32
    )
    att[my_head * seqs + my_seq] = (blended / den).astype(BF16)

    for dz, dy in others:
        send_att(z_at[dz] + y_at[dy]).start()

    all_but_one(att, 2).wait_recv()

    loads["out_weight"].wait()
    part_t = jnp.zeros((out_weight.shape[0], rows), F32)
    for h in range(heads):
        part_t += dot_last(
            out_weight[:, h * head : (h + 1) * head],
            att[pl.ds(h * seqs, seqs)].reshape(rows, head),
        )
    half = out_weight.shape[0] // 2
    low, high = part_t[:half].astype(BF16), part_t[half:].astype(BF16)
    swap_send[...] = jnp.where(core == 0, high, low)
    swap = pltpu.make_async_remote_copy(
        src_ref=swap_send,
        dst_ref=swap_recv,
        send_sem=send_sem.at[3],
        recv_sem=recv_sem.at[3],
        device_id={"tp": 1 - core},
        device_id_type=MESH,
    )
    swap.start()
    kept = jnp.where(core == 0, low, high).astype(F32)
    swap.wait()
    final = kept + swap_recv[...].astype(F32)
    result[...] = final.T.astype(BF16).reshape(seqs, props, half)

    all_but_one(o_send, 0).wait_send()
    all_but_one(lse_recv, 1).wait_send()
    all_but_one(att, 2).wait_send()


def shards(
    tokens,
    norm_gain,
    query_weight,
    key_weight,
    value_weight,
    forget_weight,
    forget_bias,
    query_gain,
    key_gain,
    output_weight,
    cache_keys,
    cache_values,
    cache_logcum,
    pending_keys,
    pending_values,
    pending_logcum,
    lengths,
    accepted,
    parents,
):
    seqs, props, width = tokens.shape
    head = query_gain.shape[0]
    heads = query_weight.shape[1] // head
    block = cache_keys.shape[1]
    taken = pending_keys.shape[1]
    rows = seqs * props
    peers = seqs * heads
    half = output_weight.shape[1] // 2
    operands = {
        "tokens": tokens.reshape(rows, width),
        "norm_gain": norm_gain.reshape(1, width),
        "query_weight": query_weight,
        "key_weight": key_weight,
        "value_weight": value_weight,
        "forget": forget_weight.T,
        "forget_bias": forget_bias,
        "query_gain": query_gain.reshape(1, head),
        "key_gain": key_gain.reshape(1, head),
        "out_weight": output_weight.T,
        "keys": cache_keys.reshape(seqs, block, head),
        "values": cache_values.reshape(seqs, block, head),
        "logcum": jnp.swapaxes(cache_logcum, 1, 2),
        "pending_keys": pending_keys.reshape(seqs, taken, head),
        "pending_values": pending_values.reshape(seqs, taken, head),
        "pending_logcum": jnp.transpose(pending_logcum, (1, 2, 0)),
        "lengths": lengths,
        "accepted": accepted,
        "accepted_row": accepted.reshape(1, seqs),
        "parents": parents,
    }
    places = {
        name: (pltpu.SMEM if name in SCALARS else pltpu.VMEM)(array.shape, array.dtype)
        for name, array in operands.items()
        if name != "value_weight"
    }
    places["key_weight"] = pltpu.VMEM((width, 2 * head), BF16)
    return pl.pallas_call(
        functools.partial(kernel, seqs, heads, props, head, taken, block),
        out_shape=jax.ShapeDtypeStruct((seqs, props, half), BF16),
        in_specs=[{name: pl.BlockSpec(memory_space=pltpu.HBM) for name in operands}],
        out_specs=pl.BlockSpec(memory_space=pltpu.VMEM),
        scratch_shapes=[
            places,
            pltpu.VMEM((rows, width), BF16),
            pltpu.VMEM((rows, 128), F32),
            pltpu.VMEM((seqs, heads * props, head), BF16),
            pltpu.VMEM((rows, head), BF16),
            pltpu.VMEM((rows, head), BF16),
            pltpu.VMEM((rows, min(rows, 128)), BF16),
            pltpu.VMEM((rows, 2 * heads), F32),
            pltpu.VMEM((peers, props, head), BF16),
            pltpu.VMEM((peers + 8, props, head), BF16),
            pltpu.VMEM((seqs, 1, 128), F32),
            pltpu.VMEM((peers + 8, 1, 128), F32),
            pltpu.VMEM((heads * props, head), F32),
            pltpu.VMEM((peers, props, head), BF16),
            pltpu.VMEM((half, rows), BF16),
            pltpu.VMEM((half, rows), BF16),
            pltpu.SemaphoreType.DMA((len(operands),)),
            pltpu.SemaphoreType.DMA((4,)),
            pltpu.SemaphoreType.DMA((4,)),
        ],
        compiler_params=pltpu.CompilerParams(
            collective_id=0, has_side_effects=True, vmem_limit_bytes=48 * 1024 * 1024
        ),
    )(
        {
            name: pltpu.with_memory_space_constraint(array, pltpu.HBM)
            for name, array in operands.items()
        }
    )


def solution(mesh):
    placed = (
        P("dp", None, None),
        P(),
        P(None, "tp"),
        P(None, "tp"),
        P(None, "tp"),
        P(),
        P(),
        P(),
        P(),
        P("tp", "kv"),
        P("dp", "kv", "tp", None),
        P("dp", "kv", "tp", None),
        P("dp", "kv", "tp"),
        P("dp", None, "tp", None),
        P("dp", None, "tp", None),
        P("dp", None, "tp"),
        P("dp"),
        P("dp"),
        P("dp", None),
    )
    return jax.shard_map(
        shards, mesh=mesh, in_specs=placed, out_specs=P("dp", None, ("kv", "tp")), check_vma=False
    )
```

```python
import functools

import jax
import jax.numpy as jnp
from jax import lax
from jax.experimental import pallas as pl
from jax.experimental.pallas import tpu as pltpu
from jax.sharding import PartitionSpec as P

EPSILON = 1e-06
NEG_LARGE = -1e30
NEG_FLOOR = -1e29
ROUNDS = (2, 2, 2, 2)
HIGHEST = lax.Precision.HIGHEST
MESH = pl.DeviceIdType.MESH
F32 = jnp.float32
BF16 = jnp.bfloat16
LAST = (((1,), (1,)), ((), ()))
NAMES = (
    "tokens",
    "norm_gain",
    "query_weight",
    "key_weight",
    "value_weight",
    "forget",
    "forget_bias",
    "query_gain",
    "key_gain",
    "out_weight",
    "keys",
    "values",
    "logcum",
    "pending_keys",
    "pending_values",
    "pending_logcum",
    "lengths",
    "accepted",
    "accepted_row",
    "parents",
)
SCALARS = ("forget_bias", "lengths", "accepted")
LOAD_ORDER = (
    "parents",
    "tokens",
    "norm_gain",
    "forget",
    "forget_bias",
    "accepted_row",
    "pending_logcum",
    "key_gain",
    "query_gain",
    "key_weight",
    "value_weight",
    "query_weight",
    "keys",
    "logcum",
    "lengths",
    "values",
    "accepted",
    "pending_keys",
    "pending_values",
    "out_weight",
)


def iota(shape, dim):
    return lax.broadcasted_iota(jnp.int32, shape, dim)


def dot_last(a, b):
    return lax.dot_general(a, b, LAST, preferred_element_type=F32)


def by_distance(count):
    return sorted(range(count), key=lambda d: -min(d, count - d))


def unit(rows, gain):
    return rows * lax.rsqrt(jnp.mean(rows * rows, axis=-1, keepdims=True) + EPSILON) * gain


def kernel(
    seqs,
    heads,
    props,
    head,
    taken,
    block,
    operands,
    result,
    places,
    normed,
    scale_scr,
    q_scr,
    kn_scr,
    vn_scr,
    anc_scr,
    cum_scr,
    o_send,
    o_recv,
    lse_send,
    lse_recv,
    tree_scr,
    att,
    swap_send,
    swap_recv,
    load_sem,
    send_sem,
    recv_sem,
):
    rows = seqs * props
    peers = seqs * heads
    scaling = head**-0.5
    me = lax.axis_index("kv")
    core = lax.axis_index("tp")
    across_y = 2 * heads
    planes = seqs // 2
    my_z = me // across_y
    my_y = me & (across_y - 1)
    my_seq = me // heads
    my_head = me & (heads - 1)
    z_at = [((my_z + dz) & (planes - 1)) * across_y for dz in range(planes)]
    y_at = [(my_y + dy) & (across_y - 1) for dy in range(across_y)]
    others = sorted(
        ((dz, dy) for dz in range(planes) for dy in range(across_y) if dz or dy),
        key=lambda d: -min(d[0], planes - d[0]) - min(d[1], across_y - d[1]),
    )

    wkv = places["key_weight"]
    places = dict(
        places, key_weight=wkv.at[:, pl.ds(0, head)], value_weight=wkv.at[:, pl.ds(head, head)]
    )
    loads = {
        name: pltpu.make_async_copy(operands[name], places[name], load_sem.at[n])
        for n, name in enumerate(LOAD_ORDER)
    }
    for item in loads.values():
        item.start()
    (
        tok, norm_gain, wq, _, _, forget, forget_bias, query_gain, key_gain, out_weight,
        kbuf, vbuf, logcum, pending_keys, pending_values, pending_logcum, lengths, accepted,
        accepted_row, parents,
    ) = (places[name] for name in NAMES)

    barrier = pltpu.get_barrier_semaphore()

    for dz, dy in others:
        pl.semaphore_signal(
            barrier, inc=1, device_id={"kv": z_at[dz] + y_at[dy]}, device_id_type=MESH
        )
    pl.semaphore_signal(barrier, inc=1, device_id={"tp": 1 - core}, device_id_type=MESH)

    loads["parents"].wait()

    lane = iota((seqs, rows), 1)
    spread = ((iota((props, rows), 1) & (props - 1)) == iota((props, rows), 0)).astype(BF16)
    repeated = jnp.dot(
        parents[...].astype(F32).astype(BF16), spread, preferred_element_type=F32
    )
    parent_row = jnp.sum(
        jnp.where(lane // props == iota((seqs, rows), 0), repeated, 0.0), axis=0, keepdims=True
    ).astype(jnp.int32)
    side = anc_scr.shape[1]
    down = iota((side, side), 0)
    across = iota((side, side), 1)
    same = down // props == across // props
    anc_t = []
    for start in range(0, rows, side):
        linked = (same & (parent_row[:, start : start + side] == (down & (props - 1)))) | (
            down == across
        )
        reach = jnp.where(linked, 1.0, 0.0).astype(BF16)
        for _ in range((props - 1).bit_length()):
            reach = jnp.minimum(
                jnp.dot(reach, reach, preferred_element_type=F32), 1.0
            ).astype(BF16)
        anc_scr[start : start + side, :] = reach
        anc_t.append(reach)

    loads["tokens"].wait()
    loads["norm_gain"].wait()

    model = tok.shape[1]

    @pl.loop(0, rows // 32)
    def _(step):
        piece = pl.ds(step * 32, 32)
        total = jnp.zeros((32, 128), F32)
        for c in range(model // 128):
            wide = tok[piece, c * 128 : (c + 1) * 128].astype(F32)
            total += wide * wide
        scale_scr[piece, :] = total

    mean = jnp.sum(scale_scr[...], axis=1, keepdims=True) * (1.0 / model)
    scale_scr[...] = jnp.broadcast_to(lax.rsqrt(mean + EPSILON), (rows, 128))

    @pl.loop(0, rows // 32)
    def _(step):
        piece = pl.ds(step * 32, 32)
        scale = scale_scr[piece, :]
        for c in range(model // 128):
            columns = slice(c * 128, (c + 1) * 128)
            wide = tok[piece, columns].astype(F32)
            normed[piece, columns] = (wide * scale * norm_gain[:, columns]).astype(BF16)

    for name in (
        "forget", "forget_bias", "accepted_row", "pending_logcum", "key_gain", "query_gain",
        "key_weight", "value_weight", "query_weight",
    ):
        loads[name].wait()
    gate_raw = dot_last(forget[...], normed[...])
    gate_head = iota((2 * heads, 1), 0)
    bias = jnp.zeros((2 * heads, 1), F32)
    for n in range(2 * heads):
        bias = jnp.where(gate_head == n, forget_bias[n], bias)
    gate_raw = gate_raw + bias
    gates = jnp.minimum(gate_raw, 0.0) - jnp.log1p(jnp.exp(-jnp.abs(gate_raw)))
    gates = jnp.where(
        core == 0, gates, jnp.concatenate([gates[heads:], gates[:heads]], axis=0)
    )
    base = jnp.zeros((heads, seqs), F32)
    for a in range(taken):
        base = jnp.where(accepted_row[...] - 1 == a, pending_logcum[a], base)
    base = jnp.concatenate([base, jnp.zeros((heads, seqs), F32)], axis=0)
    expand = (lane // props == iota((seqs, rows), 0)).astype(F32)
    cum_t = jnp.concatenate(
        [
            jnp.dot(
                gates[:, n * side : (n + 1) * side],
                reach.astype(F32),
                precision=HIGHEST,
                preferred_element_type=F32,
            )
            for n, reach in enumerate(anc_t)
        ],
        axis=1,
    ) + jnp.dot(base, expand, precision=HIGHEST, preferred_element_type=F32)
    cum_scr[...] = cum_t.T

    sides = jnp.dot(normed[...], wkv[...], preferred_element_type=F32)
    kn_scr[...] = unit(sides[:, :head], key_gain[...]).astype(BF16)
    vn_scr[...] = sides[:, head:].astype(BF16)
    for pair in range(heads // 2):
        raw = jnp.dot(
            normed[...],
            wq[:, 2 * pair * head : (2 * pair + 2) * head],
            preferred_element_type=F32,
        )
        for h in (2 * pair, 2 * pair + 1):
            one = raw[:, (h - 2 * pair) * head : (h - 2 * pair + 1) * head]
            q_scr[:, h * props : (h + 1) * props, :] = (
                unit(one, query_gain[...]).astype(BF16).reshape(seqs, props, head)
            )

    o_recv[pl.ds(peers, 8)] = jnp.zeros((8, props, head), BF16)
    lse_recv[pl.ds(peers, 8)] = jnp.full((8, 1, 128), NEG_LARGE, F32)

    for name in ("keys", "logcum", "lengths", "values"):
        loads[name].wait()
    def send_out(k):
        return pltpu.make_async_remote_copy(
            src_ref=o_send.at[k],
            dst_ref=o_recv.at[me],
            send_sem=send_sem.at[0],
            recv_sem=recv_sem.at[0],
            device_id={"kv": k},
            device_id_type=MESH,
        )

    def send_lse(k):
        return pltpu.make_async_remote_copy(
            src_ref=lse_send.at[lax.shift_right_logical(k, heads.bit_length() - 1)],
            dst_ref=lse_recv.at[me],
            send_sem=send_sem.at[1],
            recv_sem=recv_sem.at[1],
            device_id={"kv": k},
            device_id_type=MESH,
        )

    def send_att(k):
        mine = att.at[my_head * seqs + my_seq]
        return pltpu.make_async_remote_copy(
            src_ref=mine,
            dst_ref=mine,
            send_sem=send_sem.at[2],
            recv_sem=recv_sem.at[2],
            device_id={"kv": k},
            device_id_type=MESH,
        )

    def all_but_one(ref, n):
        some = ref.at[pl.ds(0, peers - 1)]
        return pltpu.make_async_remote_copy(
            src_ref=some,
            dst_ref=some,
            send_sem=send_sem.at[n],
            recv_sem=recv_sem.at[n],
            device_id={"kv": me},
            device_id_type=MESH,
        )

    def send_planes(fars):
        for far in fars:
            for dy in by_distance(across_y):
                if far or dy:
                    send_lse(z_at[far] + y_at[dy]).start()
                    send_out(z_at[far] + y_at[dy]).start()

    place = me * block + iota((1, block), 1)
    slot = iota((heads * props, 128), 1)
    late = my_z >= planes // 2
    far_first = by_distance(planes)
    far_rounds = [
        far_first[sum(ROUNDS[:g]) * planes // 8 : sum(ROUNDS[: g + 1]) * planes // 8]
        for g in range(len(ROUNDS))
    ]
    members = [
        [
            lax.shift_right_logical(z_at[far], heads.bit_length() - 1) + half
            for far in fars
            for half in range(2)
        ]
        for fars in far_rounds
    ]
    ahead = [dot_last(q_scr[s], kbuf[s]) for s in members[0]]
    for g, fars in enumerate(far_rounds):
        raws = ahead
        ahead = [dot_last(q_scr[s], kbuf[s]) for s in members[g + 1]] if g + 1 < len(members) else []
        cols = jnp.zeros((heads * props, 128), F32)
        for j, (s, raw) in enumerate(zip(members[g], raws)):
            minus = jnp.where(place < lengths[s], -logcum[s], NEG_LARGE)
            cum = cum_scr[pl.ds(pl.multiple_of(s * props, props), props), :]
            scores = jnp.concatenate(
                [
                    raw[h * props : (h + 1) * props] * scaling
                    + (cum[:, h : h + 1] + minus[h : h + 1])
                    for h in range(heads)
                ],
                axis=0,
            )
            top = jnp.maximum(jnp.max(scores, axis=-1, keepdims=True), NEG_FLOOR)
            weights = jnp.exp(scores - top)
            total = jnp.sum(weights, axis=-1, keepdims=True)
            out = jnp.dot(weights.astype(BF16), vbuf[s], preferred_element_type=F32)
            out = (out * (1.0 / jnp.maximum(total, 1.0))).astype(BF16)
            o_send[pl.ds(s * heads, heads)] = out.reshape(heads, props, head)
            cols = jnp.where(slot == j, top, jnp.where(slot == 16 + j, total, cols))
        turned = jnp.concatenate(
            [cols, jnp.zeros((128 - heads * props, 128), F32)], axis=0
        ).T
        totals = turned[16:32]
        lse_rows = jnp.where(
            totals > 0.0, turned[:16] + jnp.log(jnp.maximum(totals, 1.0)), NEG_LARGE
        )
        for j, s in enumerate(members[g]):
            lse_send[s] = lse_rows[j : j + 1]

        @pl.when(late)
        def _():
            if g == 0:
                pl.semaphore_wait(barrier, peers)
            send_planes(fars)

    @pl.when(jnp.logical_not(late))
    def _():
        pl.semaphore_wait(barrier, peers)
        send_planes(far_first)

    o_recv[me] = o_send[me]
    lse_recv[me] = lse_send[my_seq]

    for name in ("accepted", "pending_keys", "pending_values"):
        loads[name].wait()
    width = heads * props
    q_own = q_scr[my_seq]
    own_rows = pl.ds(pl.multiple_of(my_seq * props, props), props)
    extra = 16
    pad = jnp.zeros((extra - taken, head), F32)
    keys_x = jnp.concatenate(
        [
            kn_scr[own_rows, :].astype(F32),
            pending_keys[my_seq].astype(F32),
            pad,
        ],
        axis=0,
    ).astype(BF16)
    values_x = jnp.concatenate(
        [
            vn_scr[own_rows, :].astype(F32),
            pending_values[my_seq].astype(F32),
            pad,
        ],
        axis=0,
    ).astype(BF16)
    raw_t = dot_last(keys_x, q_own)
    cum_own = cum_scr[own_rows, :]
    lane_head = iota((props, width), 1) // props
    lane_prop = iota((props, width), 1) & (props - 1)
    cum_wide = jnp.zeros((props, width), F32)
    for h in range(heads):
        cum_wide = jnp.where(lane_head == h, cum_own[:, h : h + 1], cum_wide)
    cum_row = jnp.sum(
        jnp.where(lane_prop == iota((props, width), 0), cum_wide, 0.0), axis=0, keepdims=True
    )
    anc_fold = (
        (iota((side, width), 0) & (props - 1)) == (iota((side, width), 1) & (props - 1))
    ).astype(BF16)
    anc_own = jnp.dot(anc_scr[own_rows, :], anc_fold, preferred_element_type=F32)
    pend_wide = jnp.zeros((extra, width), F32)
    pend_sub = iota((extra, width), 0)
    for a in range(taken):
        col = jnp.sum(
            jnp.where(iota((heads, seqs), 1) == my_seq, pending_logcum[a], 0.0),
            axis=1,
            keepdims=True,
        )
        row = jnp.sum(
            jnp.where(iota((heads, width), 1) // props == iota((heads, width), 0), col, 0.0),
            axis=0,
            keepdims=True,
        )
        pend_wide = jnp.where(pend_sub == a, row, pend_wide)
    tree_t = jnp.where(
        anc_own > 0.5, raw_t[:props] * scaling + cum_row - cum_wide, NEG_LARGE
    )
    pend_t = jnp.where(
        pend_sub < accepted[my_seq], raw_t[props:] * scaling + cum_row - pend_wide, NEG_LARGE
    )
    both_t = jnp.concatenate([tree_t, pend_t], axis=0)
    top_t = jnp.max(both_t, axis=0, keepdims=True)
    weights_t = jnp.exp(both_t - top_t)
    total_t = jnp.sum(weights_t, axis=0, keepdims=True)
    share_t = (weights_t * (1.0 / total_t)).astype(BF16)
    tree_scr[...] = lax.dot_general(
        share_t, values_x, (((0,), (0,)), ((), ())), preferred_element_type=F32
    )
    head_rows = pl.ds(pl.multiple_of(my_head * props, props), props)
    o_recv[peers] = tree_scr[head_rows, :].astype(BF16)
    lse_t = top_t + jnp.log(total_t)
    lse_recv[peers] = jnp.concatenate([lse_t, jnp.zeros((1, 128 - width), F32)], axis=1)

    slots = peers + 8
    pick = (
        (iota((128, 128), 0) - my_head * props) == (iota((128, 128), 1) & (props - 1))
    ).astype(BF16)
    mine_8 = iota((8, 128), 1) // props == iota((8, 128), 0)
    mine_16 = (iota((props, 128), 1) & (props - 1)) == iota((props, 128), 0)
    all_but_one(lse_recv, 1).wait_recv()
    lse_all = lse_recv[:, 0, :]
    weight = jnp.exp(lse_all - jnp.max(lse_all, axis=0, keepdims=True)).astype(BF16)
    picked = jnp.dot(weight, pick, preferred_element_type=F32)
    mixes = []
    for c in range(slots // 8):
        flat = jnp.sum(
            jnp.where(mine_8, picked[c * 8 : (c + 1) * 8], 0.0), axis=0, keepdims=True
        )
        mixes.append(jnp.where(mine_16, flat, 0.0))
    den = functools.reduce(lambda a, b: a + b, mixes)
    den = jnp.sum(den, axis=1, keepdims=True)
    mix = jnp.concatenate(mixes, axis=1).astype(BF16)
    all_but_one(o_recv, 0).wait_recv()
    blended = jnp.dot(
        mix, o_recv[...].reshape(slots * props, head), preferred_element_type=F32
    )
    att[my_head * seqs + my_seq] = (blended / den).astype(BF16)

    for dz, dy in others:
        send_att(z_at[dz] + y_at[dy]).start()

    all_but_one(att, 2).wait_recv()

    loads["out_weight"].wait()
    part_t = jnp.zeros((out_weight.shape[0], rows), F32)
    for h in range(heads):
        part_t += dot_last(
            out_weight[:, h * head : (h + 1) * head],
            att[pl.ds(h * seqs, seqs)].reshape(rows, head),
        )
    half = out_weight.shape[0] // 2
    low, high = part_t[:half].astype(BF16), part_t[half:].astype(BF16)
    swap_send[...] = jnp.where(core == 0, high, low)
    swap = pltpu.make_async_remote_copy(
        src_ref=swap_send,
        dst_ref=swap_recv,
        send_sem=send_sem.at[3],
        recv_sem=recv_sem.at[3],
        device_id={"tp": 1 - core},
        device_id_type=MESH,
    )
    swap.start()
    kept = jnp.where(core == 0, low, high).astype(F32)
    swap.wait()
    final = kept + swap_recv[...].astype(F32)
    result[...] = final.T.astype(BF16).reshape(seqs, props, half)

    all_but_one(o_send, 0).wait_send()
    all_but_one(lse_recv, 1).wait_send()
    all_but_one(att, 2).wait_send()


def shards(
    tokens,
    norm_gain,
    query_weight,
    key_weight,
    value_weight,
    forget_weight,
    forget_bias,
    query_gain,
    key_gain,
    output_weight,
    cache_keys,
    cache_values,
    cache_logcum,
    pending_keys,
    pending_values,
    pending_logcum,
    lengths,
    accepted,
    parents,
):
    seqs, props, width = tokens.shape
    head = query_gain.shape[0]
    heads = query_weight.shape[1] // head
    block = cache_keys.shape[1]
    taken = pending_keys.shape[1]
    rows = seqs * props
    peers = seqs * heads
    half = output_weight.shape[1] // 2
    operands = {
        "tokens": tokens.reshape(rows, width),
        "norm_gain": norm_gain.reshape(1, width),
        "query_weight": query_weight,
        "key_weight": key_weight,
        "value_weight": value_weight,
        "forget": forget_weight.T,
        "forget_bias": forget_bias,
        "query_gain": query_gain.reshape(1, head),
        "key_gain": key_gain.reshape(1, head),
        "out_weight": output_weight.T,
        "keys": cache_keys.reshape(seqs, block, head),
        "values": cache_values.reshape(seqs, block, head),
        "logcum": jnp.swapaxes(cache_logcum, 1, 2),
        "pending_keys": pending_keys.reshape(seqs, taken, head),
        "pending_values": pending_values.reshape(seqs, taken, head),
        "pending_logcum": jnp.transpose(pending_logcum, (1, 2, 0)),
        "lengths": lengths,
        "accepted": accepted,
        "accepted_row": accepted.reshape(1, seqs),
        "parents": parents,
    }
    places = {
        name: (pltpu.SMEM if name in SCALARS else pltpu.VMEM)(array.shape, array.dtype)
        for name, array in operands.items()
        if name != "value_weight"
    }
    places["key_weight"] = pltpu.VMEM((width, 2 * head), BF16)
    return pl.pallas_call(
        functools.partial(kernel, seqs, heads, props, head, taken, block),
        out_shape=jax.ShapeDtypeStruct((seqs, props, half), BF16),
        in_specs=[{name: pl.BlockSpec(memory_space=pltpu.HBM) for name in operands}],
        out_specs=pl.BlockSpec(memory_space=pltpu.VMEM),
        scratch_shapes=[
            places,
            pltpu.VMEM((rows, width), BF16),
            pltpu.VMEM((rows, 128), F32),
            pltpu.VMEM((seqs, heads * props, head), BF16),
            pltpu.VMEM((rows, head), BF16),
            pltpu.VMEM((rows, head), BF16),
            pltpu.VMEM((rows, min(rows, 128)), BF16),
            pltpu.VMEM((rows, 2 * heads), F32),
            pltpu.VMEM((peers, props, head), BF16),
            pltpu.VMEM((peers + 8, props, head), BF16),
            pltpu.VMEM((seqs, 1, 128), F32),
            pltpu.VMEM((peers + 8, 1, 128), F32),
            pltpu.VMEM((heads * props, head), F32),
            pltpu.VMEM((peers, props, head), BF16),
            pltpu.VMEM((half, rows), BF16),
            pltpu.VMEM((half, rows), BF16),
            pltpu.SemaphoreType.DMA((len(operands),)),
            pltpu.SemaphoreType.DMA((4,)),
            pltpu.SemaphoreType.DMA((4,)),
        ],
        compiler_params=pltpu.CompilerParams(
            collective_id=0, has_side_effects=True, vmem_limit_bytes=48 * 1024 * 1024
        ),
    )(
        {
            name: pltpu.with_memory_space_constraint(array, pltpu.HBM)
            for name, array in operands.items()
        }
    )


def solution(mesh):
    placed = (
        P("dp", None, None),
        P(),
        P(None, "tp"),
        P(None, "tp"),
        P(None, "tp"),
        P(),
        P(),
        P(),
        P(),
        P("tp", "kv"),
        P("dp", "kv", "tp", None),
        P("dp", "kv", "tp", None),
        P("dp", "kv", "tp"),
        P("dp", None, "tp", None),
        P("dp", None, "tp", None),
        P("dp", None, "tp"),
        P("dp"),
        P("dp"),
        P("dp", None),
    )
    return jax.shard_map(
        shards, mesh=mesh, in_specs=placed, out_specs=P("dp", None, ("kv", "tp")), check_vma=False
    )
```
